512 devices in a mesh: sp: 64 (over z, y), tp: 8 (over x, core).
Axes of the slice: x: 4, y: 8, z: 8, core: 2. Of those that a mesh axis runs over, the one named last changes fastest.
Arguments:
- tokens: bfloat16 [16384, 1024], P(('sp', 'tp')), may hold values from -16 to 16, as said below
- valid_len: int32 [1], replicated, may hold values from 12288 to 16384
- norm_gain: float32 [1024], replicated, may hold values from 0.5 to 1.5
- w_query: bfloat16 [1024, 4096], P(None, 'tp'), may hold values from -0.1875 to 0.1875
- w_key: bfloat16 [1024, 1024], P(None, 'tp'), may hold values from -0.1875 to 0.1875
- w_value: bfloat16 [1024, 1024], P(None, 'tp'), may hold values from -0.1875 to 0.1875
- q_gain: float32 [128], replicated, may hold values from 0.5 to 1.5
- k_gain: float32 [128], replicated, may hold values from 0.5 to 1.5
- w_out: bfloat16 [4096, 1024], P('tp'), may hold values from -0.375 to 0.375
Outputs:
- mixed: bfloat16 [16384, 1024], P(('sp', 'tp'))
The draws below stay inside these ranges and needn't reach their ends.
Inputs may be any that keep to these rules, and one draw needn't show every extreme that they name: tokens are random entries of unit-order spread (normal or uniform) plus a shift shared by every run of 256 consecutive rows, within -16 and 16. valid_len is at least three quarters of 16384 and at most 16384.
All inputs are finite; a program needn't handle non-finite values.
Results may differ from the reference program's by a relative error of at most 0.02.
Values may be sent and summed in bfloat16 or wider, within the bound.
A program may use at most 64 MiB of HBM per device.

```python
import jax
import jax.numpy as jnp
from jax import lax

D = 1024
HEAD_DIM = 128
KV_HEADS = 8
Q_PER_KV = 4
GRID_W = 64
TOK_DEV = 256
Q_HEADS = 32
TOKENS = 16384
N_SP = 64


def draw_tokens(key, part):
    noise_key = jax.random.fold_in(key, 11)
    shift_key = jax.random.fold_in(key, 12)
    groups = TOKENS // TOK_DEV
    noise_part = jax.random.normal(noise_key, (TOKENS, D), jnp.float32)
    shifts = 1.5 * jax.random.normal(shift_key, (groups, D), jnp.float32)
    shifted = noise_part + jnp.repeat(shifts, TOK_DEV, axis=0)
    return jnp.clip(shifted, -16.0, 16.0).astype(jnp.bfloat16)


def levels(rng, extent, cuts, low, top_value):
    def one(axis_at, parts):
        draws = jax.random.uniform(jax.random.fold_in(jax.random.fold_in(rng, 6), axis_at), (parts,), jnp.float32, low / len(cuts), top_value / len(cuts))
        return jnp.repeat(jnp.exp(draws), extent[axis_at] // parts).reshape((-1,) + (1,) * (len(extent) - axis_at - 1))

    level = one(*cuts[0])
    for cut in cuts[1:]:
        level = level * one(*cut)
    return level


def scatter_about(rng, dims, spread, limit, cuts=(), kind=jnp.bfloat16):
    level = levels(rng, dims, cuts, -0.22, 0.18) if cuts else 1.0
    drawn = jax.random.normal(rng, dims, jnp.float32) * spread * level
    return jnp.minimum(jnp.maximum(drawn, -limit), limit).astype(kind)


def setup_inputs(seed: int = 0) -> dict:
    seeds = jax.random.split(jax.random.key(seed), 10)
    tokens = draw_tokens(jax.random.fold_in(seeds[9], 71), 0)
    valid_len = jax.random.randint(seeds[1], (1,), TOKENS * 3 // 4, TOKENS + 1).astype(jnp.int32)
    norm_gain = jnp.clip(1.0 + 0.1 * jax.random.normal(seeds[2], (D,), jnp.float32), 0.5, 1.5)
    w_query = scatter_about(seeds[3], (D, Q_HEADS * HEAD_DIM), D ** -0.5, 0.1875, ((1, 8),))
    w_key = scatter_about(seeds[4], (D, KV_HEADS * HEAD_DIM), D ** -0.5, 0.1875, ((1, 8),))
    w_value = scatter_about(seeds[5], (D, KV_HEADS * HEAD_DIM), D ** -0.5, 0.1875, ((1, 8),))
    q_gain = jnp.clip(1.0 + 0.1 * jax.random.normal(seeds[6], (HEAD_DIM,), jnp.float32), 0.5, 1.5)
    k_gain = jnp.clip(1.0 + 0.1 * jax.random.normal(seeds[7], (HEAD_DIM,), jnp.float32), 0.5, 1.5)
    w_out = scatter_about(seeds[8], (Q_HEADS * HEAD_DIM, D), (Q_HEADS * HEAD_DIM // 16) ** -0.5, 0.375, ((0, 8),))
    return dict(tokens=tokens, valid_len=valid_len, norm_gain=norm_gain, w_query=w_query, w_key=w_key, w_value=w_value, q_gain=q_gain, k_gain=k_gain, w_out=w_out)


norm_eps = 1e-06
rope_base = 10000.0

def normalize(values, gain):
    scaled = values.astype(jnp.float32)
    return scaled * lax.rsqrt(lax.optimization_barrier(jnp.mean(scaled * scaled, axis=-1, keepdims=True)) + norm_eps) * gain

def rope_tables(positions, head_width):
    quarter = head_width // 4
    half_width = head_width // 2
    frequency = rope_base ** (-(jnp.arange(quarter, dtype=jnp.float32) * 2.0) / half_width)
    grid_row = (positions // GRID_W).astype(jnp.float32)
    grid_col = (positions % GRID_W).astype(jnp.float32)
    row_angle = grid_row[:, None] * frequency[None, :]
    col_angle = grid_col[:, None] * frequency[None, :]
    angles = jnp.concatenate([row_angle, row_angle, col_angle, col_angle], axis=-1)
    return (jnp.cos(angles), jnp.sin(angles))

def turn_half(values):
    width = values.shape[-1] // 2
    return jnp.concatenate([-values[..., width:], values[..., :width]], axis=-1)

def prepare(projected, gain, positions, factor):
    head_width = gain.shape[0]
    shaped = projected.astype(jnp.float32).reshape(projected.shape[0], -1, head_width)
    unit = normalize(shaped, gain)
    half_width = head_width // 2
    turned = jnp.concatenate([turn_half(unit[..., :half_width]), turn_half(unit[..., half_width:])], axis=-1)
    cosine, sine_table = rope_tables(positions, head_width)
    result = unit * cosine[:, None, :] + turned * sine_table[:, None, :]
    return (result * factor).astype(jnp.bfloat16)

def reference(tokens, valid_len, norm_gain, w_query, w_key, w_value, q_gain, k_gain, w_out):
    normed = normalize(tokens, norm_gain).astype(jnp.bfloat16)
    queries = jnp.dot(normed, w_query, preferred_element_type=jnp.float32).astype(jnp.bfloat16)
    keys_all = jnp.dot(normed, w_key, preferred_element_type=jnp.float32).astype(jnp.bfloat16)
    values = jnp.dot(normed, w_value, preferred_element_type=jnp.float32).astype(jnp.bfloat16)
    positions = jnp.arange(TOKENS, dtype=jnp.int32)
    turned_query = lax.optimization_barrier(prepare(queries, q_gain, positions, HEAD_DIM ** (-0.5)))
    turned_key = lax.optimization_barrier(prepare(keys_all, k_gain, positions, 1.0))
    key_wide = turned_key.astype(jnp.float32)
    value_wide = values.reshape(TOKENS, KV_HEADS, HEAD_DIM).astype(jnp.float32)
    key_valid = positions < valid_len[0]
    grouped = turned_query.reshape(N_SP, TOK_DEV, KV_HEADS, Q_PER_KV, HEAD_DIM)

    def attend(query_block):
        scores = jnp.einsum('qgrd,kgd->grqk', query_block.astype(jnp.float32), key_wide)
        scores = jnp.where(key_valid[None, None, None, :], scores, -jnp.inf)
        top = lax.optimization_barrier(jnp.max(scores, axis=-1, keepdims=True))
        weights = jnp.exp(scores - top)
        totals = lax.optimization_barrier(jnp.sum(weights, axis=-1))
        rounded = lax.optimization_barrier(weights.astype(jnp.bfloat16))
        summed = jnp.einsum('grqk,kgd->grqd', rounded.astype(jnp.float32), value_wide)
        result = summed / totals[..., None]
        return result.transpose(2, 0, 1, 3).reshape(TOK_DEV, Q_HEADS * HEAD_DIM).astype(jnp.bfloat16)
    attended = lax.map(attend, grouped).reshape(TOKENS, Q_HEADS * HEAD_DIM)
    return jnp.dot(attended, w_out, preferred_element_type=jnp.float32).astype(jnp.bfloat16)
```

```python
import functools
import math

import jax
import jax.numpy as jnp
from jax import lax
from jax.experimental import pallas as pl
from jax.experimental.pallas import tpu as pltpu
from jax.sharding import PartitionSpec as P

HEAD_DIM = 128
Q_PER_KV = 4
GRID_W = 64
ROWS = 32
BLOCK = 256
HALF = 128
RING = 8
MODEL = 1024

norm_eps = 1e-06
rope_base = 10000.0
MESH = pl.DeviceIdType.MESH


def unit_rows(rows, gain):
    wide = rows.astype(jnp.float32)
    scale = lax.rsqrt(jnp.mean(wide * wide, axis=-1, keepdims=True) + norm_eps)
    return (wide * scale * gain).astype(jnp.bfloat16)


def rotate(part, tables):
    width = part.shape[-1]
    scale = lax.rsqrt(jnp.mean(part * part, axis=-1, keepdims=True) + norm_eps)
    ahead = pltpu.roll(part, width // 4, 1)
    behind = pltpu.roll(part, width - width // 4, 1)
    return (part * tables[0] + ahead * tables[1] + behind * tables[2]) * scale


def kernel(valid_ref, own_ref, gain_ref, gains_ref, w_query_hbm, w_key_hbm, w_value_hbm,
           w_out_hbm, out_ref,
           tok, units, ones, q_scr, acc, att, tabs, w_query, w_key, w_value, w_out,
           give, take, part, landed,
           load_sem, tok_send, tok_recv, unit_recv, near_send, far_send, end_send, end_recv):
    me = lax.axis_index("sp")
    tp = lax.axis_index("tp")
    z, y = me // RING, me % RING
    x, core = tp // 2, tp % 2
    x_up, x_down, x_far = (x + 1) % 4, (x + 3) % 4, (x + 2) % 4
    to_mate = {"sp": me, "tp": 2 * x + 1 - core}

    def along_x(at):
        return {"sp": me, "tp": 2 * at + core}

    to_zy = [
        [{"sp": ((z + 1) % RING) * RING + y, "tp": tp},
         {"sp": ((z + RING - 1) % RING) * RING + y, "tp": tp}],
        [{"sp": z * RING + (y + 1) % RING, "tp": tp},
         {"sp": z * RING + (y + RING - 1) % RING, "tp": tp}],
    ]

    loads = [
        pltpu.make_async_copy(src, dst, load_sem.at[i])
        for i, (src, dst) in enumerate([
            (w_key_hbm, w_key), (w_value_hbm, w_value), (w_query_hbm, w_query),
            (w_out_hbm, w_out)])
    ]
    for load in loads:
        load.start()

    barrier = pltpu.get_barrier_semaphore()
    friends = [to_mate, along_x(x_up), along_x(x_down), along_x(x_far)]
    friends += to_zy[0] + to_zy[1]
    for friend in friends:
        pl.semaphore_signal(barrier, inc=1, device_id=friend, device_id_type=MESH)
    pl.semaphore_wait(barrier, len(friends))

    def remote(source, target, send, recv, device):
        return pltpu.make_async_remote_copy(
            src_ref=source, dst_ref=target, send_sem=send, recv_sem=recv,
            device_id=device, device_id_type=MESH)

    def row_of(at, side):
        return pl.multiple_of(side * HALF + at * ROWS, ROWS)

    def rows_at(at, side):
        return tok.at[pl.ds(row_of(at, side), ROWS), :]

    def half_rows(at, which):
        start = pl.multiple_of(core * HALF + at * ROWS + which * (ROWS // 2), ROWS // 2)
        return tok.at[pl.ds(start, ROWS // 2), :]

    mine = rows_at(x, core)
    tok_up = remote(own_ref, mine, tok_send.at[0], tok_recv.at[0], along_x(x_up))
    tok_down = remote(own_ref, mine, tok_send.at[1], tok_recv.at[1], along_x(x_down))
    tok_mate = remote(own_ref, mine, tok_send.at[2], tok_recv.at[2], to_mate)
    tok_up.start()
    tok_down.start()
    tok_mate.start()
    tok[pl.ds(row_of(x, core), ROWS), :] = own_ref[...]

    lane = lax.broadcasted_iota(jnp.int32, (BLOCK, HEAD_DIM), 1)
    line = lax.broadcasted_iota(jnp.int32, (BLOCK, HEAD_DIM), 0)
    grid_row = me * 4 + (line % HALF) // ROWS
    grid_col = (line // HALF) * ROWS + line % ROWS
    spot = jnp.where(lane < HEAD_DIM // 2, grid_row, grid_col).astype(jnp.float32)
    exponent = (lane % 32).astype(jnp.float32) * (-2.0 / 64 * math.log2(rope_base))
    angle = spot * jnp.exp2(exponent)
    cosine, sine = jnp.cos(angle), jnp.sin(angle)
    second = (lane // 32) % 2 == 1
    tabs[0] = cosine
    tabs[1] = jnp.where(second, sine, 0.0)
    tabs[2] = jnp.where(second, 0.0, -sine)

    valid = valid_ref[0]
    short = lax.broadcasted_iota(jnp.int32, (HALF, HEAD_DIM), 0)
    spread = short + (short // ROWS) * ROWS

    def fill(p, carry):
        for side in range(2):
            kept = spread + (p * BLOCK + side * ROWS) < valid
            ones[2 * p + side] = jnp.where(kept, 1.0, 0.0).astype(jnp.bfloat16)
        return carry

    lax.fori_loop(0, RING * RING, fill, 0)
    acc[...] = jnp.zeros_like(acc)

    fwd_up = remote(half_rows(x_down, 0), half_rows(x_down, 0), tok_send.at[3], tok_recv.at[3],
                    along_x(x_up))
    fwd_down = remote(half_rows(x_up, 1), half_rows(x_up, 1), tok_send.at[4], tok_recv.at[4],
                      along_x(x_down))

    def to_partner(at, slot):
        return remote(rows_at(at, core), rows_at(at, core), tok_send.at[slot],
                      tok_recv.at[slot], to_mate)

    share_down, share_up, share_far = to_partner(x_down, 5), to_partner(x_up, 6), to_partner(x_far, 7)
    tok_up.wait_recv()
    fwd_up.start()
    share_down.start()
    tok_down.wait_recv()
    fwd_down.start()
    share_up.start()
    tok_mate.wait_recv()
    fwd_up.wait_recv()
    fwd_down.wait_recv()
    share_far.start()
    share_down.wait_recv()
    share_up.wait_recv()
    share_far.wait_recv()

    normed = unit_rows(tok[...], gain_ref[...])
    loads[0].wait()
    loads[1].wait()
    turn = [tabs[i] for i in range(3)]
    k_tables = [turn[i] * gains_ref[3 + i:4 + i, :] for i in range(3)]
    keys = rotate(jnp.dot(normed, w_key[...], preferred_element_type=jnp.float32), k_tables)
    values = jnp.dot(normed, w_value[...], preferred_element_type=jnp.float32)
    for side in range(2):
        rows = slice(side * HALF, (side + 1) * HALF)
        kept = spread + (me * BLOCK + side * ROWS) < valid
        units[2 * me + side, :HALF, :] = keys[rows].T.astype(jnp.bfloat16)
        units[2 * me + side, HALF:, :] = jnp.where(kept, values[rows], 0.0).astype(jnp.bfloat16)

    coords = [z, y]

    def unit_at(side, s, t):
        block = s * RING + t if side == 0 else t * RING + s
        return 2 * block + side

    def relay(unit, device, send):
        return remote(units.at[unit], units.at[unit], send, unit_recv.at[unit], device)

    def await_unit(unit):
        remote(units.at[unit], units.at[unit], near_send.at[0], unit_recv.at[unit],
               to_mate).wait_recv()

    def chain(d, sign):
        return jnp.maximum(2 * d - 1 + sign, 0)

    def source(side, d, sign):
        return (coords[side] + d * (2 * sign - 1) + RING) % RING

    def near_copy(side, way, d, unit):
        return relay(unit, to_zy[side][way], near_send.at[(side * 2 + way) * 4 + d])

    def far_copy(side, way, j, k, unit):
        return relay(unit, to_zy[1 - side][way], far_send.at[((side * 2 + way) * 8 + j) * 4 + k])

    def near_sends(side, way, d):
        even = 1 - coords[1 - side] % 2 if way == 0 else coords[1 - side] % 2
        return jnp.logical_or(d < 3, jnp.logical_and(d == 3, even == 1))

    def far_sends(side, way, s, k):
        even = 1 - s % 2 if way == 0 else s % 2
        return jnp.logical_or(k < 3, jnp.logical_and(k == 3, even == 1))

    for side in range(2):
        unit = unit_at(side, coords[side], coords[1 - side])
        for way in range(2):
            near_copy(side, way, 0, unit).start()
            far_copy(side, way, 0, 0, unit).start()

    loads[2].wait()
    q_tables = [turn[i] * gains_ref[i:i + 1, :] for i in range(3)]
    projected = jnp.dot(normed, w_query[...], preferred_element_type=jnp.float32)
    for r in range(Q_PER_KV):
        head = rotate(projected[:, r * HEAD_DIM:(r + 1) * HEAD_DIM], q_tables)
        q_scr[r] = head.astype(jnp.bfloat16)

    def arrive(d, sign):
        for side in range(2):
            unit = unit_at(side, source(side, d, sign), coords[1 - side])
            await_unit(unit)
            for way in range(2):
                far_copy(side, way, chain(d, sign), 0, unit).start()

                @pl.when(jnp.logical_and(sign == way, near_sends(side, way, d)))
                def _():
                    near_copy(side, way, d, unit).start()

    def attend(picks):
        key = jnp.concatenate([units[u, :HALF, :] for u in picks], axis=1)
        val = jnp.concatenate([units[u, HALF:, :] for u in picks], axis=0)
        one = jnp.concatenate([ones[u] for u in picks], axis=0)
        both = jnp.concatenate([val, one], axis=1)
        for r in range(Q_PER_KV):
            scores = jnp.dot(q_scr[r], key, preferred_element_type=jnp.float32)
            weights = jnp.exp2(scores).astype(jnp.bfloat16)
            acc[r] += jnp.dot(weights, both, preferred_element_type=jnp.float32)

    def event(i, state):
        d, sign, k = state

        @pl.when(jnp.logical_and(k == 1, jnp.logical_or(d < 3, jnp.logical_and(d == 3, sign == 0))))
        def _():
            arrive(d + 1, sign)

        @pl.when(jnp.logical_and(k == 1, d == 0))
        def _():
            arrive(d + 1, sign + 1)

        picks = []
        for side in range(2):
            s = source(side, d, sign)
            t = coords[1 - side]
            lower = unit_at(side, s, (t + RING - k) % RING)
            upper = unit_at(side, s, (t + k * (1 - k // 4)) % RING)
            await_unit(lower)

            @pl.when(far_sends(side, 0, s, k))
            def _():
                far_copy(side, 0, chain(d, sign), k, lower).start()

            @pl.when(k < 4)
            def _():
                await_unit(upper)

                @pl.when(far_sends(side, 1, s, k))
                def _():
                    far_copy(side, 1, chain(d, sign), k, upper).start()

            picks += [lower, upper]
        attend(picks)

        flip = jnp.where(jnp.logical_and(sign == 0, jnp.logical_and(d > 0, d < 4)), 1, 0)
        within = jnp.where(jnp.logical_and(d > 0, k < 4), 1, 0)
        top = jnp.minimum(4, d + k)
        d_next = flip * d + (1 - flip) * (within * (d - 1) + (1 - within) * top)
        k_next = flip * k + (1 - flip) * (within * (k + 1) + (1 - within) * (d + k + 1 - top))
        return d_next, flip, k_next

    zero = jnp.int32(0)
    lax.fori_loop(0, 32, event, (zero, zero, zero + 1))

    for r in range(Q_PER_KV):
        att[:, r * HEAD_DIM:(r + 1) * HEAD_DIM] = (
            acc[r, :, :HEAD_DIM] / acc[r, :, HEAD_DIM:]
        ).astype(jnp.bfloat16)

    loads[3].wait()
    theirs = pl.multiple_of((1 - core) * HALF, HALF)
    ours = pl.multiple_of(core * HALF, HALF)
    give[...] = jnp.dot(
        att[pl.ds(theirs, HALF), :], w_out[...], preferred_element_type=jnp.float32
    ).astype(jnp.bfloat16)
    swap = remote(give, take, end_send.at[0], end_recv.at[0], to_mate)
    swap.start()
    kept_sum = jnp.dot(att[pl.ds(ours, HALF), :], w_out[...], preferred_element_type=jnp.float32)
    swap.wait_recv()
    part[...] = kept_sum + take[...].astype(jnp.float32)
    swap.wait_send()
    sends = []
    for i, at in enumerate([x_far, x_up, x_down]):
        here = pl.ds(pl.multiple_of(at * ROWS, ROWS), ROWS)
        give[here, :] = part[here, :].astype(jnp.bfloat16)
        sends.append(remote(give.at[here, :], landed.at[i], end_send.at[1 + i],
                            end_recv.at[1 + i], along_x(at)))
        sends[-1].start()

    for copy in (tok_up, tok_down, tok_mate, fwd_up, fwd_down, share_down, share_up, share_far):
        copy.wait_send()

    def settle(j, carry):
        d = (j + 1) // 2
        sign = jnp.where(j > 0, (j + 1) % 2, 0)
        for side in range(2):
            s = source(side, d, sign)
            unit = unit_at(side, s, coords[1 - side])
            for way in range(2):
                for k in range(4):
                    @pl.when(far_sends(side, way, s, k))
                    def _():
                        far_copy(side, way, j, k, unit).wait_send()

                @pl.when(jnp.logical_and(
                    jnp.logical_or(j == 0, sign == way), near_sends(side, way, d)))
                def _():
                    near_copy(side, way, d, unit).wait_send()
        return carry

    lax.fori_loop(0, 8, settle, 0)
    total = part[pl.ds(pl.multiple_of(x * ROWS, ROWS), ROWS), :]
    for i, copy in enumerate(sends):
        copy.wait_recv()
        total = total + landed[i].astype(jnp.float32)
    for copy in sends:
        copy.wait_send()
    out_ref[...] = total.astype(jnp.bfloat16)


def on_device(tokens, valid_len, norm_gain, w_query, w_key, w_value, q_gain, k_gain, w_out):
    factor = HEAD_DIM ** (-0.5) * math.log2(math.e)

    def three(gain):
        return [gain, jnp.roll(gain, 32), jnp.roll(gain, -32)]

    blank = jnp.zeros_like(q_gain)
    gains = jnp.stack(three(q_gain * factor) + three(k_gain) + [blank, blank])
    vmem = pl.BlockSpec(memory_space=pltpu.VMEM)
    smem = pl.BlockSpec(memory_space=pltpu.SMEM)
    hbm = pl.BlockSpec(memory_space=pl.ANY)
    dma = pltpu.SemaphoreType.DMA
    bf16, f32 = jnp.bfloat16, jnp.float32
    n_units = 2 * RING * RING
    return pl.pallas_call(
        kernel,
        out_shape=jax.ShapeDtypeStruct(tokens.shape, bf16),
        in_specs=[smem, vmem, vmem, vmem, hbm, hbm, hbm, hbm],
        out_specs=vmem,
        scratch_shapes=[
            pltpu.VMEM((BLOCK, MODEL), bf16),
            pltpu.VMEM((n_units, BLOCK, HEAD_DIM), bf16),
            pltpu.VMEM((n_units, HALF, HEAD_DIM), bf16),
            pltpu.VMEM((Q_PER_KV, BLOCK, HEAD_DIM), bf16),
            pltpu.VMEM((Q_PER_KV, BLOCK, 2 * HEAD_DIM), f32),
            pltpu.VMEM((BLOCK, Q_PER_KV * HEAD_DIM), bf16),
            pltpu.VMEM((3, BLOCK, HEAD_DIM), f32),
            pltpu.VMEM(w_query.shape, bf16),
            pltpu.VMEM(w_key.shape, bf16),
            pltpu.VMEM(w_value.shape, bf16),
            pltpu.VMEM(w_out.shape, bf16),
            pltpu.VMEM((HALF, MODEL), bf16),
            pltpu.VMEM((HALF, MODEL), bf16),
            pltpu.VMEM((HALF, MODEL), f32),
            pltpu.VMEM((3, ROWS, MODEL), bf16),
            dma((4,)), dma((8,)), dma((8,)), dma((n_units,)), dma((16,)), dma((128,)),
            dma((4,)), dma((4,)),
        ],
        compiler_params=pltpu.CompilerParams(
            collective_id=0, has_side_effects=True, vmem_limit_bytes=60 * 1024 * 1024),
    )(valid_len, tokens, norm_gain[None, :], gains, w_query, w_key, w_value, w_out)


def solution(mesh):
    return jax.shard_map(
        on_device,
        mesh=mesh,
        in_specs=(
            P(("sp", "tp"), None),
            P(),
            P(),
            P(None, "tp"),
            P(None, "tp"),
            P(None, "tp"),
            P(),
            P(),
            P("tp", None),
        ),
        out_specs=P(("sp", "tp"), None),
        check_vma=False,
    )
```

```python
import functools
import math

import jax
import jax.numpy as jnp
from jax import lax
from jax.experimental import pallas as pl
from jax.experimental.pallas import tpu as pltpu
from jax.sharding import PartitionSpec as P

HEAD_DIM = 128
Q_PER_KV = 4
GRID_W = 64
ROWS = 32
BLOCK = 256
HALF = 128
RING = 8
MODEL = 1024

norm_eps = 1e-06
rope_base = 10000.0
MESH = pl.DeviceIdType.MESH


def unit_rows(rows, gain):
    wide = rows.astype(jnp.float32)
    scale = lax.rsqrt(jnp.mean(wide * wide, axis=-1, keepdims=True) + norm_eps)
    return (wide * scale * gain).astype(jnp.bfloat16)


def rotate(part, tables):
    width = part.shape[-1]
    scale = lax.rsqrt(jnp.mean(part * part, axis=-1, keepdims=True) + norm_eps)
    ahead = pltpu.roll(part, width // 4, 1)
    behind = pltpu.roll(part, width - width // 4, 1)
    return (part * tables[0] + ahead * tables[1] + behind * tables[2]) * scale


def kernel(valid_ref, own_hbm, gain_hbm, q_gain_hbm, k_gain_hbm, w_query_hbm, w_key_hbm,
           w_value_hbm, w_out_hbm, out_ref,
           own, gain, q_gain, k_gain, tok, units, ones, q_scr, acc, att, tabs,
           w_query, w_key, w_value, w_out, o_give, o_take, give, take, part, landed,
           load_sem, tok_send, tok_recv, unit_recv, near_send, far_send, pair_send, pair_recv,
           end_send, end_recv):
    me = lax.axis_index("sp")
    tp = lax.axis_index("tp")
    z, y = me // RING, me % RING
    x, core = tp // 2, tp % 2
    x_up, x_down, x_far = (x + 1) % 4, (x + 3) % 4, (x + 2) % 4
    to_mate = {"sp": me, "tp": 2 * x + 1 - core}
    a = core * y + (1 - core) * z
    b = core * z + (1 - core) * y
    parity, group = a % 2, a // 2

    def block_at(a_at, b_at):
        return (1 - core) * (a_at * RING + b_at) + core * (b_at * RING + a_at)

    def along_x(at):
        return {"sp": me, "tp": 2 * at + core}

    def along(a_at, b_at):
        return {"sp": block_at(a_at, b_at), "tp": tp}

    to_near = [along(2 * ((group + 1) % 4) + parity, b), along(2 * ((group + 3) % 4) + parity, b)]
    to_far = [along(a, (b + 1) % RING), along(a, (b + RING - 1) % RING)]
    to_pair = along(a + 1 - 2 * parity, b)

    barrier = pltpu.get_barrier_semaphore()
    friends = [to_mate, along_x(x_far), along_x(x_up), along_x(x_down), to_pair]
    friends += to_near + to_far
    for friend in friends:
        pl.semaphore_signal(barrier, inc=1, device_id=friend, device_id_type=MESH)

    loads = [
        pltpu.make_async_copy(src, dst, load_sem.at[i])
        for i, (src, dst) in enumerate([
            (own_hbm, own), (gain_hbm, gain), (k_gain_hbm, k_gain), (q_gain_hbm, q_gain),
            (w_key_hbm, w_key), (w_value_hbm, w_value), (w_query_hbm, w_query),
            (w_out_hbm, w_out)])
    ]
    for load in loads:
        load.start()
    loads[0].wait()
    pl.semaphore_wait(barrier, len(friends))

    def remote(source, target, send, recv, device):
        return pltpu.make_async_remote_copy(
            src_ref=source, dst_ref=target, send_sem=send, recv_sem=recv,
            device_id=device, device_id_type=MESH)

    def row_of(at, side):
        return pl.multiple_of(side * HALF + at * ROWS, ROWS)

    def rows_at(at, side):
        return tok.at[pl.ds(row_of(at, side), ROWS), :]

    mine = rows_at(x, core)
    tok_far = remote(own, mine, tok_send.at[0], tok_recv.at[0], along_x(x_far))
    tok_up = remote(own, mine, tok_send.at[1], tok_recv.at[1], along_x(x_up))
    tok_down = remote(own, mine, tok_send.at[2], tok_recv.at[2], along_x(x_down))
    tok_mate = remote(own, mine, tok_send.at[3], tok_recv.at[3], to_mate)
    tok_copies = [tok_far, tok_up, tok_down, tok_mate]
    for copy in tok_copies:
        copy.start()
    tok[pl.ds(row_of(x, core), ROWS), :] = own[...]

    lane = lax.broadcasted_iota(jnp.int32, (BLOCK, HEAD_DIM), 1)
    line = lax.broadcasted_iota(jnp.int32, (BLOCK, HEAD_DIM), 0)
    grid_row = me * 4 + (line % HALF) // ROWS
    grid_col = (line // HALF) * ROWS + line % ROWS
    spot = jnp.where(lane < HEAD_DIM // 2, grid_row, grid_col).astype(jnp.float32)
    exponent = (lane % 32).astype(jnp.float32) * (-2.0 / 64 * math.log2(rope_base))
    angle = spot * jnp.exp2(exponent)
    cosine, sine = jnp.cos(angle), jnp.sin(angle)
    second = (lane // 32) % 2 == 1
    tabs[0] = cosine
    tabs[1] = jnp.where(second, sine, 0.0)
    tabs[2] = jnp.where(second, 0.0, -sine)

    def share(at, slot):
        return remote(rows_at(at, core), rows_at(at, core), tok_send.at[slot],
                      tok_recv.at[slot], to_mate)

    shares = [share(x_far, 4), share(x_down, 5), share(x_up, 6)]
    for copy, onward in ((tok_up, shares[1]), (tok_down, shares[2]), (tok_far, shares[0])):
        copy.wait_recv()
        onward.start()

    valid = valid_ref[0]
    short = lax.broadcasted_iota(jnp.int32, (HALF, HEAD_DIM), 0)
    spread = short + (short // ROWS) * ROWS
    for i in range(1, 6):
        loads[i].wait()

    def turns(table, side):
        wide = jnp.broadcast_to(table, (8, HEAD_DIM))
        moved = [wide, pltpu.roll(wide, 32, 1), pltpu.roll(wide, HEAD_DIM - 32, 1)]
        rows = pl.ds(pl.multiple_of(side * HALF, HALF), HALF)
        return [tabs[i, rows, :] * moved[i][:1, :] for i in range(3)]

    def unit_at(group_at, b_at, side):
        return (group_at * RING + b_at) * 2 + side

    def relay(unit, device, send):
        return remote(units.at[unit], units.at[unit], send, unit_recv.at[unit], device)

    def await_unit(unit):
        relay(unit, to_mate, near_send.at[0]).wait_recv()

    def near_copy(way, d, side, unit):
        return relay(unit, to_near[way], near_send.at[(way * 2 + d) * 2 + side])

    def far_copy(way, j, k, side, unit):
        return relay(unit, to_far[way], far_send.at[((way * 4 + j) * 4 + k) * 2 + side])

    def project(side):
        rows = pl.ds(pl.multiple_of(side * HALF, HALF), HALF)
        normed = unit_rows(tok[rows, :], gain[...])
        keys = rotate(jnp.dot(normed, w_key[...], preferred_element_type=jnp.float32),
                      turns(k_gain[...], side))
        values = jnp.dot(normed, w_value[...], preferred_element_type=jnp.float32)
        kept = spread + (me * BLOCK + side * ROWS) < valid
        unit = unit_at(group, b, side)
        units[unit, :HALF, :] = keys.T.astype(jnp.bfloat16)
        units[unit, HALF:, :] = jnp.where(kept, values, 0.0).astype(jnp.bfloat16)
        for way in range(2):
            far_copy(way, 0, 0, side, unit).start()
            near_copy(way, 0, side, unit).start()
        return normed

    def queries(normed, side):
        rows = pl.ds(pl.multiple_of(side * HALF, HALF), HALF)
        factor = HEAD_DIM ** (-0.5) * math.log2(math.e)
        tables = turns(q_gain[...] * factor, side)
        projected = jnp.dot(normed, w_query[...], preferred_element_type=jnp.float32)
        for r in range(Q_PER_KV):
            head = rotate(projected[:, r * HEAD_DIM:(r + 1) * HEAD_DIM], tables)
            q_scr[r, rows, :] = head.astype(jnp.bfloat16)

    first = project(core)
    tok_mate.wait_recv()
    for copy in shares:
        copy.wait_recv()
    other = project(1 - core)
    loads[6].wait()
    queries(first, core)
    queries(other, 1 - core)
    q_swap = remote(q_scr.at[pl.ds(0, 4)], q_scr.at[pl.ds(4, 4)], pair_send.at[0],
                    pair_recv.at[0], to_pair)
    q_swap.start()

    def fill(i, carry):
        p = block_at(2 * (i // RING) + parity, i % RING)
        for side in range(2):
            kept = spread + (p * BLOCK + side * ROWS) < valid
            ones[2 * i + side] = jnp.where(kept, 1.0, 0.0).astype(jnp.bfloat16)
        return carry

    lax.fori_loop(0, 4 * RING, fill, 0)
    acc[...] = jnp.zeros_like(acc)

    def chain(d, sign):
        return jnp.maximum(2 * d - 1 + sign, 0)

    def source(d, sign):
        return (group + d * (2 * sign - 1) + 4) % 4

    def arrive(d, sign):
        for side in range(2):
            unit = unit_at(source(d, sign), b, side)
            await_unit(unit)
            for way in range(2):
                far_copy(way, chain(d, sign), 0, side, unit).start()

            @pl.when(jnp.logical_and(d == 1, sign == side))
            def _():
                near_copy(side, 1, side, unit).start()

    def attend(picks, heads):
        key = jnp.concatenate([units[u, :HALF, :] for u in picks], axis=1)
        val = jnp.concatenate([units[u, HALF:, :] for u in picks], axis=0)
        one = jnp.concatenate([ones[u] for u in picks], axis=0)
        both = jnp.concatenate([val, one], axis=1)
        for r in heads:
            scores = jnp.dot(q_scr[r], key, preferred_element_type=jnp.float32)
            weights = jnp.exp2(scores).astype(jnp.bfloat16)
            acc[r] += jnp.dot(weights, both, preferred_element_type=jnp.float32)

    def event(i, state):
        d, sign, k = state

        @pl.when(jnp.logical_and(k == 1, jnp.logical_and(d < 2, sign == 0)))
        def _():
            arrive(d + 1, sign)

        @pl.when(jnp.logical_and(k == 1, d == 0))
        def _():
            arrive(d + 1, sign + 1)

        s = source(d, sign)
        low, high = (b + RING - k) % RING, (b + k) % RING
        for side in range(2):
            for way, at in enumerate((low, high)):
                unit = unit_at(s, at, side)

                @pl.when(jnp.logical_or(k < 4, side == way))
                def _():
                    await_unit(unit)

                @pl.when(jnp.logical_or(k < 3, jnp.logical_and(k == 3, side == way)))
                def _():
                    far_copy(way, chain(d, sign), k, side, unit).start()

        last = k // 4
        second = last * b + (1 - last) * high
        picks = [unit_at(s, at, side) for at in (low, second) for side in range(2)]

        @pl.when(i == 0)
        def _():
            q_swap.wait_recv()

        attend(picks, range(8))

        flip = jnp.where(jnp.logical_and(sign == 0, d == 1), 1, 0)
        within = jnp.where(jnp.logical_and(d > 0, k < 4), 1, 0)
        top = jnp.minimum(2, d + k)
        d_next = flip * d + (1 - flip) * (within * (d - 1) + (1 - within) * top)
        k_next = flip * k + (1 - flip) * (within * (k + 1) + (1 - within) * (d + k + 1 - top))
        return d_next, flip, k_next

    zero = jnp.int32(0)
    lax.fori_loop(0, 16, event, (zero, zero, zero + 1))

    small = lax.broadcasted_iota(jnp.int32, (BLOCK, HEAD_DIM), 1) // 32
    sums = acc[4, :, HEAD_DIM:]
    for r in range(Q_PER_KV):
        o_give[:, r * HEAD_DIM:(r + 1) * HEAD_DIM] = acc[4 + r, :, :HEAD_DIM].astype(jnp.bfloat16)
        sums = jnp.where(small == r, acc[4 + r, :, HEAD_DIM:], sums)
    o_give[:, 4 * HEAD_DIM:] = sums.astype(jnp.bfloat16)
    o_swap = remote(o_give, o_take, pair_send.at[1], pair_recv.at[1], to_pair)
    o_swap.start()

    def settle(j, carry):
        d = (j + 1) // 2
        sign = jnp.where(j > 0, (j + 1) % 2, 0)
        s = source(d, sign)
        for side in range(2):
            unit = unit_at(s, b, side)
            for way in range(2):
                for k in range(4 if side == way else 3):
                    far_copy(way, j, k, side, unit).wait_send()

                @pl.when(j == 0)
                def _():
                    near_copy(way, 0, side, unit).wait_send()

            @pl.when(jnp.logical_and(d == 1, sign == side))
            def _():
                near_copy(side, 1, side, unit).wait_send()
        return carry

    lax.fori_loop(0, 4, settle, 0)
    for copy in tok_copies + shares + [q_swap]:
        copy.wait_send()
    loads[7].wait()
    o_swap.wait_recv()
    for r in range(Q_PER_KV):
        span = slice(r * HEAD_DIM, (r + 1) * HEAD_DIM)
        total = acc[r, :, HEAD_DIM:] + o_take[
            :, 4 * HEAD_DIM + 32 * r:4 * HEAD_DIM + 32 * r + 1].astype(jnp.float32)
        att[:, span] = (
            (acc[r, :, :HEAD_DIM] + o_take[:, span].astype(jnp.float32)) / total
        ).astype(jnp.bfloat16)

    theirs = pl.multiple_of((1 - core) * HALF, HALF)
    ours = pl.multiple_of(core * HALF, HALF)
    give[...] = jnp.dot(
        att[pl.ds(theirs, HALF), :], w_out[...], preferred_element_type=jnp.float32
    ).astype(jnp.bfloat16)
    swap = remote(give, take, end_send.at[0], end_recv.at[0], to_mate)
    swap.start()
    kept_sum = jnp.dot(att[pl.ds(ours, HALF), :], w_out[...], preferred_element_type=jnp.float32)
    swap.wait_recv()
    part[...] = kept_sum + take[...].astype(jnp.float32)
    swap.wait_send()
    sends = []
    for i, at in enumerate([x_far, x_up, x_down]):
        here = pl.ds(pl.multiple_of(at * ROWS, ROWS), ROWS)
        give[here, :] = part[here, :].astype(jnp.bfloat16)
        sends.append(remote(give.at[here, :], landed.at[i], end_send.at[1 + i],
                            end_recv.at[1 + i], along_x(at)))
        sends[-1].start()

    total = part[pl.ds(pl.multiple_of(x * ROWS, ROWS), ROWS), :]
    o_swap.wait_send()
    for i, copy in enumerate(sends):
        copy.wait_recv()
        total = total + landed[i].astype(jnp.float32)
    for copy in sends:
        copy.wait_send()
    out_ref[...] = total.astype(jnp.bfloat16)


def on_device(tokens, valid_len, norm_gain, w_query, w_key, w_value, q_gain, k_gain, w_out):
    vmem = pl.BlockSpec(memory_space=pltpu.VMEM)
    smem = pl.BlockSpec(memory_space=pltpu.SMEM)
    hbm = pl.BlockSpec(memory_space=pl.ANY)
    dma = pltpu.SemaphoreType.DMA
    bf16, f32 = jnp.bfloat16, jnp.float32
    n_units = RING * RING
    return pl.pallas_call(
        kernel,
        out_shape=jax.ShapeDtypeStruct(tokens.shape, bf16),
        in_specs=[smem] + [hbm] * 8,
        out_specs=vmem,
        scratch_shapes=[
            pltpu.VMEM(tokens.shape, bf16),
            pltpu.VMEM((1, MODEL), f32),
            pltpu.VMEM((1, HEAD_DIM), f32),
            pltpu.VMEM((1, HEAD_DIM), f32),
            pltpu.VMEM((BLOCK, MODEL), bf16),
            pltpu.VMEM((n_units, BLOCK, HEAD_DIM), bf16),
            pltpu.VMEM((n_units, HALF, HEAD_DIM), bf16),
            pltpu.VMEM((2 * Q_PER_KV, BLOCK, HEAD_DIM), bf16),
            pltpu.VMEM((2 * Q_PER_KV, BLOCK, 2 * HEAD_DIM), f32),
            pltpu.VMEM((BLOCK, Q_PER_KV * HEAD_DIM), bf16),
            pltpu.VMEM((3, BLOCK, HEAD_DIM), f32),
            pltpu.VMEM(w_query.shape, bf16),
            pltpu.VMEM(w_key.shape, bf16),
            pltpu.VMEM(w_value.shape, bf16),
            pltpu.VMEM(w_out.shape, bf16),
            pltpu.VMEM((BLOCK, 5 * HEAD_DIM), bf16),
            pltpu.VMEM((BLOCK, 5 * HEAD_DIM), bf16),
            pltpu.VMEM((HALF, MODEL), bf16),
            pltpu.VMEM((HALF, MODEL), bf16),
            pltpu.VMEM((HALF, MODEL), f32),
            pltpu.VMEM((3, ROWS, MODEL), bf16),
            dma((8,)), dma((8,)), dma((8,)), dma((n_units,)), dma((8,)), dma((64,)),
            dma((2,)), dma((2,)), dma((4,)), dma((4,)),
        ],
        compiler_params=pltpu.CompilerParams(
            collective_id=0, has_side_effects=True, vmem_limit_bytes=60 * 1024 * 1024),
    )(valid_len, tokens, norm_gain[None, :], q_gain[None, :], k_gain[None, :], w_query, w_key,
      w_value, w_out)


def solution(mesh):
    return jax.shard_map(
        on_device,
        mesh=mesh,
        in_specs=(
            P(("sp", "tp"), None),
            P(),
            P(),
            P(None, "tp"),
            P(None, "tp"),
            P(None, "tp"),
            P(),
            P(),
            P("tp", None),
        ),
        out_specs=P(("sp", "tp"), None),
        check_vma=False,
    )
```

```python
import functools
import math

import jax
import jax.numpy as jnp
from jax import lax
from jax.experimental import pallas as pl
from jax.experimental.pallas import tpu as pltpu
from jax.sharding import PartitionSpec as P

HEAD_DIM = 128
Q_PER_KV = 4
GRID_W = 64
ROWS = 32
BLOCK = 256
HALF = 128
RING = 8
MODEL = 1024

LATE = 6
ORDER = [
    (0, 0, 1, 1), (1, 1, 1, 2), (1, 0, 1, 0), (0, 0, 2, 0),
    (2, 0, 1, 0), (1, 1, 2, 0), (1, 0, 2, 0), (0, 0, 3, 0),
    (2, 0, 2, 0), (1, 1, 3, 0), (1, 0, 3, 0), (0, 0, 4, 0),
    (2, 0, 3, 0), (1, 1, 4, 0), (1, 0, 4, 0), (2, 0, 4, 0),
]

norm_eps = 1e-06
rope_base = 10000.0
MESH = pl.DeviceIdType.MESH


def unit_rows(rows, gain):
    wide = rows.astype(jnp.float32)
    scale = lax.rsqrt(jnp.mean(wide * wide, axis=-1, keepdims=True) + norm_eps)
    return (wide * scale * gain).astype(jnp.bfloat16)


def rotate(part, tables):
    width = part.shape[-1]
    scale = lax.rsqrt(jnp.mean(part * part, axis=-1, keepdims=True) + norm_eps)
    ahead = pltpu.roll(part, width // 4, 1)
    behind = pltpu.roll(part, width - width // 4, 1)
    return (part * tables[0] + ahead * tables[1] + behind * tables[2]) * scale


def kernel(valid_ref, own_hbm, gain_hbm, q_gain_hbm, k_gain_hbm, w_query_hbm, w_key_hbm,
           w_value_hbm, w_out_hbm, out_ref,
           own, gain, q_gain, k_gain, tok, units, ones, q_scr, acc, att, tabs,
           w_query, w_key, w_value, w_out, o_give, o_take, give, take, ship, landed,
           load_sem, tok_send, tok_recv, unit_recv, near_send, far_send, pair_send, pair_recv,
           end_send, end_recv):
    me = lax.axis_index("sp")
    tp = lax.axis_index("tp")
    z, y = me // RING, me % RING
    x, core = tp // 2, tp % 2
    x_up, x_down, x_far = (x + 1) % 4, (x + 3) % 4, (x + 2) % 4
    to_mate = {"sp": me, "tp": 2 * x + 1 - core}
    a = core * y + (1 - core) * z
    b = core * z + (1 - core) * y
    parity, group = a % 2, a // 2

    def block_at(a_at, b_at):
        return (1 - core) * (a_at * RING + b_at) + core * (b_at * RING + a_at)

    def along_x(at):
        return {"sp": me, "tp": 2 * at + core}

    def along(a_at, b_at):
        return {"sp": block_at(a_at, b_at), "tp": tp}

    to_near = [along(2 * ((group + 1) % 4) + parity, b), along(2 * ((group + 3) % 4) + parity, b)]
    to_far = [along(a, (b + 1) % RING), along(a, (b + RING - 1) % RING)]
    to_pair = along(a + 1 - 2 * parity, b)

    barrier = pltpu.get_barrier_semaphore()
    friends = [to_mate, along_x(x_far), along_x(x_up), along_x(x_down), to_pair]
    friends += to_near + to_far
    for friend in friends:
        pl.semaphore_signal(barrier, inc=1, device_id=friend, device_id_type=MESH)

    loads = [
        pltpu.make_async_copy(src, dst, load_sem.at[i])
        for i, (src, dst) in enumerate([
            (own_hbm, own), (gain_hbm, gain), (k_gain_hbm, k_gain), (q_gain_hbm, q_gain),
            (w_key_hbm, w_key), (w_value_hbm, w_value), (w_query_hbm, w_query),
            (w_out_hbm, w_out)])
    ]
    for load in loads:
        load.start()
    loads[0].wait()
    pl.semaphore_wait(barrier, len(friends))

    def remote(source, target, send, recv, device):
        return pltpu.make_async_remote_copy(
            src_ref=source, dst_ref=target, send_sem=send, recv_sem=recv,
            device_id=device, device_id_type=MESH)

    def slot(at):
        return tok.at[at * ROWS:(at + 1) * ROWS, :]

    tok_up = remote(own, slot(2), tok_send.at[0], tok_recv.at[0], along_x(x_up))
    tok_down = remote(own, slot(1), tok_send.at[1], tok_recv.at[1], along_x(x_down))
    tok_mate = remote(own, slot(0), tok_send.at[2], tok_recv.at[2], to_mate)
    tok_far = remote(own, slot(4), tok_send.at[3], tok_recv.at[3], along_x(x_far))
    tok_copies = [tok_up, tok_down, tok_mate, tok_far]
    for copy in tok_copies:
        copy.start()
    tok[3 * ROWS:4 * ROWS, :] = own[...]

    def place(line):
        at = line // ROWS
        ahead = jnp.where(jnp.logical_or(at == 1, at == 6), 1, 0)
        ahead = jnp.where(jnp.logical_or(at == 2, at == 7), 3, ahead)
        ahead = jnp.where(jnp.logical_or(at == 4, at == 5), 2, ahead)
        side = jnp.where(jnp.logical_and(at > 0, at < 5), core, 1 - core)
        return (x + ahead) % 4, side * ROWS + line % ROWS

    lane = lax.broadcasted_iota(jnp.int32, (BLOCK, HEAD_DIM), 1)
    line = lax.broadcasted_iota(jnp.int32, (BLOCK, HEAD_DIM), 0)
    grid_row, grid_col = place(line)
    spot = jnp.where(lane < HEAD_DIM // 2, me * 4 + grid_row, grid_col).astype(jnp.float32)
    exponent = (lane % 32).astype(jnp.float32) * (-2.0 / 64 * math.log2(rope_base))
    angle = spot * jnp.exp2(exponent)
    cosine, sine = jnp.cos(angle), jnp.sin(angle)
    second = (lane // 32) % 2 == 1
    tabs[0] = cosine
    tabs[1] = jnp.where(second, sine, 0.0)
    tabs[2] = jnp.where(second, 0.0, -sine)

    valid = valid_ref[0]
    spread = []
    for side in range(2):
        short = lax.broadcasted_iota(jnp.int32, (HALF, HEAD_DIM), 0) + side * HALF
        high, low = place(short)
        spread.append(high * GRID_W + low)
    def fill(i, carry):
        p = block_at(2 * (i // RING) + parity, i % RING)
        for side in range(2):
            kept = spread[side] + p * BLOCK < valid
            ones[2 * i + side] = jnp.where(kept, 1.0, 0.0).astype(jnp.bfloat16)
        return carry

    lax.fori_loop(0, 4 * RING, fill, 0)
    acc[...] = jnp.zeros_like(acc)

    def share(ours, theirs, at):
        return remote(slot(ours), slot(theirs), tok_send.at[at], tok_recv.at[at], to_mate)

    shares = [share(2, 7, 4), share(1, 6, 5), share(4, 5, 6)]
    for copy, onward in zip((tok_up, tok_down), shares):
        copy.wait_recv()
        onward.start()
    tok_mate.wait_recv()

    for i in range(1, 6):
        loads[i].wait()

    def turns(table, side):
        wide = jnp.broadcast_to(table, (8, HEAD_DIM))
        moved = [wide, pltpu.roll(wide, 32, 1), pltpu.roll(wide, HEAD_DIM - 32, 1)]
        rows = slice(side * HALF, (side + 1) * HALF)
        return [tabs[i, rows, :] * moved[i][:1, :] for i in range(3)]

    def unit_at(group_at, b_at, side):
        return (group_at * RING + b_at) * 2 + side

    def relay(unit, device, send):
        return remote(units.at[unit], units.at[unit], send, unit_recv.at[unit], device)

    def await_unit(unit):
        relay(unit, to_mate, near_send.at[0]).wait_recv()

    def near_copy(way, d, side, unit):
        return relay(unit, to_near[way], near_send.at[(way * 2 + d) * 2 + side])

    def far_copy(way, j, k, side, unit):
        return relay(unit, to_far[way], far_send.at[((way * 4 + j) * 4 + k) * 2 + side])

    def project(side):
        rows = slice(side * HALF, (side + 1) * HALF)
        normed = unit_rows(tok[rows, :], gain[...])
        keys = rotate(jnp.dot(normed, w_key[...], preferred_element_type=jnp.float32),
                      turns(k_gain[...], side))
        values = jnp.dot(normed, w_value[...], preferred_element_type=jnp.float32)
        kept = spread[side] + me * BLOCK < valid
        unit = unit_at(group, b, side)
        units[unit, :HALF, :] = keys.T.astype(jnp.bfloat16)
        units[unit, HALF:, :] = jnp.where(kept, values, 0.0).astype(jnp.bfloat16)
        for way in range(2):
            far_copy(way, 0, 0, side, unit).start()
            near_copy(way, 0, side, unit).start()
        return normed

    def queries(normed, side):
        rows = slice(side * HALF, (side + 1) * HALF)
        factor = HEAD_DIM ** (-0.5) * math.log2(math.e)
        tables = turns(q_gain[...] * factor, side)
        projected = jnp.dot(normed, w_query[...], preferred_element_type=jnp.float32)
        for r in range(Q_PER_KV):
            head = rotate(projected[:, r * HEAD_DIM:(r + 1) * HEAD_DIM], tables)
            q_scr[r, rows, :] = head.astype(jnp.bfloat16)

    first = project(0)
    tok_far.wait_recv()
    shares[2].start()
    for copy in shares:
        copy.wait_recv()
    other = project(1)
    loads[6].wait()
    queries(first, 0)
    queries(other, 1)
    q_swap = remote(q_scr.at[pl.ds(0, 4)], q_scr.at[pl.ds(4, 4)], pair_send.at[0],
                    pair_recv.at[0], to_pair)
    q_swap.start()

    def chain(d, sign):
        return jnp.maximum(2 * d - 1 + sign, 0)

    def source(d, sign):
        return (group + d * (2 * sign - 1) + 4) % 4

    def arrive(d, sign):
        for side in range(2):
            unit = unit_at(source(d, sign), b, side)
            await_unit(unit)
            for way in range(2):
                far_copy(way, chain(d, sign), 0, side, unit).start()

            if d == 1 and sign == side:
                near_copy(side, 1, side, unit).start()

    def attend(picks, heads):
        key = jnp.concatenate([units[u, :HALF, :] for u in picks], axis=1)
        val = jnp.concatenate([units[u, HALF:, :] for u in picks], axis=0)
        one = jnp.concatenate([ones[u] for u in picks], axis=0)
        both = jnp.concatenate([val, one], axis=1)
        def score(r):
            return jnp.dot(q_scr[r], key, preferred_element_type=jnp.float32)

        heads = list(heads)
        ahead = score(heads[0])
        for at, r in enumerate(heads):
            weights = jnp.exp2(ahead).astype(jnp.bfloat16)
            if at + 1 < len(heads):
                ahead = score(heads[at + 1])
            acc[r] += jnp.dot(weights, both, preferred_element_type=jnp.float32)

    def lookup(i):
        code = jnp.int32(0)
        for at, (d, sign, k, step) in enumerate(ORDER):
            code = jnp.where(i == at, ((d * 2 + sign) * 5 + k) * 4 + step, code)
        step, rest = code % 4, code // 4
        k, rest = rest % 5, rest // 5
        return rest // 2, rest % 2, k, step

    def picks_of(i):
        d, sign, k, step = lookup(i)
        s, low, high = source(d, sign), (b + RING - k) % RING, (b + k) % RING
        last = k // 4
        second = last * b + (1 - last) * high
        return [unit_at(s, at, side) for at in (low, second) for side in range(2)]

    def exchange(i):
        d, sign, k, step = lookup(i)
        s, low, high = source(d, sign), (b + RING - k) % RING, (b + k) % RING
        for side in range(2):
            for way, at in enumerate((low, high)):
                unit = unit_at(s, at, side)

                @pl.when(jnp.logical_or(k < 4, side == way))
                def _():
                    await_unit(unit)

                @pl.when(jnp.logical_or(k < 3, jnp.logical_and(k == 3, side == way)))
                def _():
                    far_copy(way, chain(d, sign), k, side, unit).start()

        @pl.when(step == 1)
        def _():
            arrive(1, 1)
            arrive(1, 0)

        @pl.when(step == 2)
        def _():
            arrive(2, 0)

    def event(i, carry):
        exchange(i)

        @pl.when(i == 0)
        def _():
            q_swap.wait_recv()

        attend(picks_of(i), range(8))
        return carry

    def late_event(i, carry):
        exchange(i)
        attend(picks_of(i), range(4, 8))
        return carry

    lax.fori_loop(0, 16 - LATE, event, 0)
    lax.fori_loop(16 - LATE, 16, late_event, 0)

    small = lax.broadcasted_iota(jnp.int32, (BLOCK, HEAD_DIM), 1) // 32
    sums = acc[4, :, HEAD_DIM:]
    for r in range(Q_PER_KV):
        o_give[:, r * HEAD_DIM:(r + 1) * HEAD_DIM] = acc[4 + r, :, :HEAD_DIM].astype(jnp.bfloat16)
        sums = jnp.where(small == r, acc[4 + r, :, HEAD_DIM:], sums)
    o_give[:, 4 * HEAD_DIM:] = sums.astype(jnp.bfloat16)
    o_swaps = [
        remote(o_give.at[low:high, :], o_take.at[low:high, :], pair_send.at[at],
               pair_recv.at[at], to_pair)
        for at, (low, high) in enumerate(((128, 192), (192, 256), (0, 128)), 1)
    ]
    for copy in o_swaps:
        copy.start()

    def settle(j, carry):
        d = (j + 1) // 2
        sign = jnp.where(j > 0, (j + 1) % 2, 0)
        s = source(d, sign)
        for side in range(2):
            unit = unit_at(s, b, side)
            for way in range(2):
                for k in range(4 if side == way else 3):
                    far_copy(way, j, k, side, unit).wait_send()

                @pl.when(j == 0)
                def _():
                    near_copy(way, 0, side, unit).wait_send()

            @pl.when(jnp.logical_and(d == 1, sign == side))
            def _():
                near_copy(side, 1, side, unit).wait_send()
        return carry

    def catch_up(i, carry):
        first = 16 - LATE + 2 * i
        attend(picks_of(first) + picks_of(first + 1), range(4))
        return carry

    lax.fori_loop(0, LATE // 2, catch_up, 0)
    lax.fori_loop(0, 4, settle, 0)
    for copy in tok_copies + shares + [q_swap]:
        copy.wait_send()
    loads[7].wait()

    def combine(low, high):
        rows = slice(low, high)
        for r in range(Q_PER_KV):
            span = slice(r * HEAD_DIM, (r + 1) * HEAD_DIM)
            lane_at = 4 * HEAD_DIM + 32 * r
            total = acc[r, rows, HEAD_DIM:] + o_take[
                rows, lane_at:lane_at + 1].astype(jnp.float32)
            att[rows, span] = (
                (acc[r, rows, :HEAD_DIM] + o_take[rows, span].astype(jnp.float32)) / total
            ).astype(jnp.bfloat16)

    def mix(low, high):
        return jnp.dot(att[low * ROWS:high * ROWS, :], w_out[...],
                       preferred_element_type=jnp.float32)

    def part_of(ref, low, high):
        return ref.at[low * ROWS:high * ROWS, :]

    o_swaps[0].wait_recv()
    combine(128, 192)
    both = mix(4, 6)
    give[3 * ROWS:, :] = both[ROWS:].astype(jnp.bfloat16)
    swap_far = remote(part_of(give, 3, 4), part_of(take, 3, 4), end_send.at[0],
                      end_recv.at[0], to_mate)
    swap_far.start()
    swap_far.wait_recv()
    ship[2 * ROWS:, :] = (both[:ROWS] + take[3 * ROWS:, :].astype(jnp.float32)).astype(jnp.bfloat16)
    out_far = remote(part_of(ship, 2, 3), landed.at[0], end_send.at[1], end_recv.at[1],
                     along_x(x_far))
    out_far.start()

    o_swaps[1].wait_recv()
    combine(192, 256)
    give[:2 * ROWS, :] = mix(6, 8).astype(jnp.bfloat16)
    o_swaps[2].wait_recv()
    combine(0, 128)
    front = mix(0, 4)
    give[2 * ROWS:3 * ROWS, :] = front[:ROWS].astype(jnp.bfloat16)
    swap = remote(part_of(give, 0, 3), part_of(take, 0, 3), end_send.at[2], end_recv.at[2],
                  to_mate)
    swap.start()
    swap.wait_recv()
    near = front[ROWS:] + take[:3 * ROWS, :].astype(jnp.float32)
    ship[:2 * ROWS, :] = near[:2 * ROWS].astype(jnp.bfloat16)
    out_up = remote(part_of(ship, 0, 1), landed.at[1], end_send.at[3], end_recv.at[3],
                    along_x(x_up))
    out_down = remote(part_of(ship, 1, 2), landed.at[2], end_send.at[4], end_recv.at[4],
                      along_x(x_down))
    out_up.start()
    out_down.start()
    total = near[2 * ROWS:]
    for copy in o_swaps + [swap_far, swap]:
        copy.wait_send()
    for i, copy in enumerate((out_far, out_up, out_down)):
        copy.wait_recv()
        total = total + landed[i].astype(jnp.float32)
    for copy in (out_far, out_up, out_down):
        copy.wait_send()
    out_ref[...] = total.astype(jnp.bfloat16)


def on_device(tokens, valid_len, norm_gain, w_query, w_key, w_value, q_gain, k_gain, w_out):
    vmem = pl.BlockSpec(memory_space=pltpu.VMEM)
    smem = pl.BlockSpec(memory_space=pltpu.SMEM)
    hbm = pl.BlockSpec(memory_space=pl.ANY)
    dma = pltpu.SemaphoreType.DMA
    bf16, f32 = jnp.bfloat16, jnp.float32
    n_units = RING * RING
    return pl.pallas_call(
        kernel,
        out_shape=pltpu.VMEM(tokens.shape, bf16),
        in_specs=[smem] + [hbm] * 8,
        out_specs=vmem,
        scratch_shapes=[
            pltpu.VMEM(tokens.shape, bf16),
            pltpu.VMEM((1, MODEL), f32),
            pltpu.VMEM((1, HEAD_DIM), f32),
            pltpu.VMEM((1, HEAD_DIM), f32),
            pltpu.VMEM((BLOCK, MODEL), bf16),
            pltpu.VMEM((n_units, BLOCK, HEAD_DIM), bf16),
            pltpu.VMEM((n_units, HALF, HEAD_DIM), bf16),
            pltpu.VMEM((2 * Q_PER_KV, BLOCK, HEAD_DIM), bf16),
            pltpu.VMEM((2 * Q_PER_KV, BLOCK, 2 * HEAD_DIM), f32),
            pltpu.VMEM((BLOCK, Q_PER_KV * HEAD_DIM), bf16),
            pltpu.VMEM((3, BLOCK, HEAD_DIM), f32),
            pltpu.VMEM(w_query.shape, bf16),
            pltpu.VMEM(w_key.shape, bf16),
            pltpu.VMEM(w_value.shape, bf16),
            pltpu.VMEM(w_out.shape, bf16),
            pltpu.VMEM((BLOCK, 5 * HEAD_DIM), bf16),
            pltpu.VMEM((BLOCK, 5 * HEAD_DIM), bf16),
            pltpu.VMEM((HALF, MODEL), bf16),
            pltpu.VMEM((HALF, MODEL), bf16),
            pltpu.VMEM((3 * ROWS, MODEL), bf16),
            pltpu.VMEM((3, ROWS, MODEL), bf16),
            dma((8,)), dma((8,)), dma((8,)), dma((n_units,)), dma((8,)), dma((64,)),
            dma((4,)), dma((4,)), dma((5,)), dma((5,)),
        ],
        compiler_params=pltpu.CompilerParams(
            collective_id=0, has_side_effects=True, vmem_limit_bytes=60 * 1024 * 1024),
    )(valid_len, tokens, norm_gain[None, :], q_gain[None, :], k_gain[None, :], w_query, w_key,
      w_value, w_out)


def solution(mesh):
    return jax.shard_map(
        on_device,
        mesh=mesh,
        in_specs=(
            P(("sp", "tp"), None),
            P(),
            P(),
            P(None, "tp"),
            P(None, "tp"),
            P(None, "tp"),
            P(),
            P(),
            P("tp", None),
        ),
        out_specs=P(("sp", "tp"), None),
        check_vma=False,
    )
```

```python
import functools
import math

import jax
import jax.numpy as jnp
from jax import lax
from jax.experimental import pallas as pl
from jax.experimental.pallas import tpu as pltpu
from jax.sharding import PartitionSpec as P

HEAD_DIM = 128
Q_PER_KV = 4
GRID_W = 64
ROWS = 32
BLOCK = 256
HALF = 128
RING = 8
MODEL = 1024

LATE = 6
EARLY = 1
ORDER = [
    (0, 0, 1, 1), (1, 1, 1, 0), (1, 0, 1, 0), (2, 0, 1, 0),
    (0, 0, 2, 0), (1, 1, 2, 0), (1, 0, 2, 0), (2, 0, 2, 0),
    (0, 0, 3, 0), (1, 1, 3, 0), (1, 0, 3, 0), (2, 0, 3, 0),
    (0, 0, 4, 0), (1, 1, 4, 0), (1, 0, 4, 0), (2, 0, 4, 0),
]

norm_eps = 1e-06
rope_base = 10000.0
MESH = pl.DeviceIdType.MESH


def unit_rows(rows, gain):
    wide = rows.astype(jnp.float32)
    scale = lax.rsqrt(jnp.mean(wide * wide, axis=-1, keepdims=True) + norm_eps)
    return (wide * scale * gain).astype(jnp.bfloat16)


def rotate(part, tables):
    width = part.shape[-1]
    scale = lax.rsqrt(jnp.mean(part * part, axis=-1, keepdims=True) + norm_eps)
    ahead = pltpu.roll(part, width // 4, 1)
    behind = pltpu.roll(part, width - width // 4, 1)
    return (part * tables[0] + ahead * tables[1] + behind * tables[2]) * scale


def kernel(valid_ref, own_hbm, gain_hbm, q_gain_hbm, k_gain_hbm, w_query_hbm, w_key_hbm,
           w_value_hbm, w_out_hbm, out_ref,
           own, gain, q_gain, k_gain, tok, units, ones, q_scr, acc, att, tabs,
           w_query, w_key, w_value, w_out, o_give, o_take, give, take, ship, landed,
           load_sem, tok_send, tok_recv, unit_recv, near_send, far_send, pair_send, pair_recv,
           end_send, end_recv):
    me = lax.axis_index("sp")
    tp = lax.axis_index("tp")
    z, y = me // RING, me % RING
    x, core = tp // 2, tp % 2
    x_up, x_down, x_far = (x + 1) % 4, (x + 3) % 4, (x + 2) % 4
    to_mate = {"sp": me, "tp": 2 * x + 1 - core}
    a = core * y + (1 - core) * z
    b = core * z + (1 - core) * y
    parity, group = a % 2, a // 2

    def block_at(a_at, b_at):
        return (1 - core) * (a_at * RING + b_at) + core * (b_at * RING + a_at)

    def along_x(at):
        return {"sp": me, "tp": 2 * at + core}

    def along(a_at, b_at):
        return {"sp": block_at(a_at, b_at), "tp": tp}

    to_near = [along(2 * ((group + ahead) % 4) + parity, b) for ahead in (1, 3, 2)]
    to_far = [along(a, (b + 1) % RING), along(a, (b + RING - 1) % RING)]
    to_pair = along(a + 1 - 2 * parity, b)

    barrier = pltpu.get_barrier_semaphore()
    friends = [to_mate, along_x(x_far), along_x(x_up), along_x(x_down), to_pair]
    friends += to_near + to_far
    for friend in friends:
        pl.semaphore_signal(barrier, inc=1, device_id=friend, device_id_type=MESH)

    loads = [
        pltpu.make_async_copy(src, dst, load_sem.at[i])
        for i, (src, dst) in enumerate([
            (own_hbm, own), (gain_hbm, gain), (k_gain_hbm, k_gain), (q_gain_hbm, q_gain),
            (w_key_hbm, w_key), (w_value_hbm, w_value), (w_query_hbm, w_query),
            (w_out_hbm, w_out)])
    ]
    for load in loads:
        load.start()
    loads[0].wait()
    pl.semaphore_wait(barrier, len(friends))

    def remote(source, target, send, recv, device):
        return pltpu.make_async_remote_copy(
            src_ref=source, dst_ref=target, send_sem=send, recv_sem=recv,
            device_id=device, device_id_type=MESH)

    def slot(at):
        return tok.at[at * ROWS:(at + 1) * ROWS, :]

    tok_up = remote(own, slot(2), tok_send.at[0], tok_recv.at[0], along_x(x_up))
    tok_down = remote(own, slot(1), tok_send.at[1], tok_recv.at[1], along_x(x_down))
    tok_mate = remote(own, slot(0), tok_send.at[2], tok_recv.at[2], to_mate)
    tok_far = remote(own, slot(4), tok_send.at[3], tok_recv.at[3], along_x(x_far))
    tok_copies = [tok_up, tok_down, tok_mate, tok_far]
    for copy in tok_copies:
        copy.start()
    tok[3 * ROWS:4 * ROWS, :] = own[...]

    def place(line):
        at = line // ROWS
        ahead = jnp.where(jnp.logical_or(at == 1, at == 6), 1, 0)
        ahead = jnp.where(jnp.logical_or(at == 2, at == 7), 3, ahead)
        ahead = jnp.where(jnp.logical_or(at == 4, at == 5), 2, ahead)
        side = jnp.where(jnp.logical_and(at > 0, at < 5), core, 1 - core)
        return (x + ahead) % 4, side * ROWS + line % ROWS

    lane = lax.broadcasted_iota(jnp.int32, (BLOCK, HEAD_DIM), 1)
    line = lax.broadcasted_iota(jnp.int32, (BLOCK, HEAD_DIM), 0)
    grid_row, grid_col = place(line)
    spot = jnp.where(lane < HEAD_DIM // 2, me * 4 + grid_row, grid_col).astype(jnp.float32)
    exponent = (lane % 32).astype(jnp.float32) * (-2.0 / 64 * math.log2(rope_base))
    angle = spot * jnp.exp2(exponent)
    cosine, sine = jnp.cos(angle), jnp.sin(angle)
    second = (lane // 32) % 2 == 1
    tabs[0] = cosine
    tabs[1] = jnp.where(second, sine, 0.0)
    tabs[2] = jnp.where(second, 0.0, -sine)

    valid = valid_ref[0]
    spread = []
    for side in range(2):
        short = lax.broadcasted_iota(jnp.int32, (HALF, HEAD_DIM), 0) + side * HALF
        high, low = place(short)
        spread.append(high * GRID_W + low)
    def fill(i, carry):
        p = block_at(2 * (i // RING) + parity, i % RING)
        for side in range(2):
            kept = spread[side] + p * BLOCK < valid
            ones[2 * i + side] = jnp.where(kept, 1.0, 0.0).astype(jnp.bfloat16)
        return carry

    lax.fori_loop(0, 4 * RING, fill, 0)
    acc[...] = jnp.zeros_like(acc)

    def share(ours, theirs, at):
        return remote(slot(ours), slot(theirs), tok_send.at[at], tok_recv.at[at], to_mate)

    shares = [share(2, 7, 4), share(1, 6, 5), share(4, 5, 6)]
    for copy, onward in zip((tok_up, tok_down), shares):
        copy.wait_recv()
        onward.start()
    tok_mate.wait_recv()

    for i in range(1, 6):
        loads[i].wait()

    def turns(table, side):
        wide = jnp.broadcast_to(table, (8, HEAD_DIM))
        moved = [wide, pltpu.roll(wide, 32, 1), pltpu.roll(wide, HEAD_DIM - 32, 1)]
        rows = slice(side * HALF, (side + 1) * HALF)
        return [tabs[i, rows, :] * moved[i][:1, :] for i in range(3)]

    def unit_at(group_at, b_at, side):
        return (group_at * RING + b_at) * 2 + side

    def relay(unit, device, send):
        return remote(units.at[unit], units.at[unit], send, unit_recv.at[unit], device)

    def await_unit(unit):
        relay(unit, to_mate, near_send.at[0]).wait_recv()

    def near_copy(way, side, unit):
        return relay(unit, to_near[way], near_send.at[way * 2 + side])

    def far_copy(way, j, k, side, unit):
        return relay(unit, to_far[way], far_send.at[((way * 4 + j) * 4 + k) * 2 + side])

    def project(side):
        rows = slice(side * HALF, (side + 1) * HALF)
        normed = unit_rows(tok[rows, :], gain[...])
        keys = rotate(jnp.dot(normed, w_key[...], preferred_element_type=jnp.float32),
                      turns(k_gain[...], side))
        values = jnp.dot(normed, w_value[...], preferred_element_type=jnp.float32)
        kept = spread[side] + me * BLOCK < valid
        unit = unit_at(group, b, side)
        units[unit, :HALF, :] = keys.T.astype(jnp.bfloat16)
        units[unit, HALF:, :] = jnp.where(kept, values, 0.0).astype(jnp.bfloat16)
        for way in range(2):
            far_copy(way, 0, 0, side, unit).start()
        for way in (0, 1, 2):
            near_copy(way, side, unit).start()
        return normed

    def queries(normed, side):
        rows = slice(side * HALF, (side + 1) * HALF)
        factor = HEAD_DIM ** (-0.5) * math.log2(math.e)
        tables = turns(q_gain[...] * factor, side)
        projected = jnp.dot(normed, w_query[...], preferred_element_type=jnp.float32)
        for r in range(Q_PER_KV):
            head = rotate(projected[:, r * HEAD_DIM:(r + 1) * HEAD_DIM], tables)
            q_scr[r, rows, :] = head.astype(jnp.bfloat16)

    first = project(0)
    tok_far.wait_recv()
    shares[2].start()
    for copy in shares:
        copy.wait_recv()
    other = project(1)
    loads[6].wait()
    queries(first, 0)
    queries(other, 1)
    q_swap = remote(q_scr.at[pl.ds(0, 4)], q_scr.at[pl.ds(4, 4)], pair_send.at[0],
                    pair_recv.at[0], to_pair)
    q_swap.start()

    def chain(d, sign):
        return jnp.maximum(2 * d - 1 + sign, 0)

    def source(d, sign):
        return (group + d * (2 * sign - 1) + 4) % 4

    def arrive(d, sign):
        for side in range(2):
            unit = unit_at(source(d, sign), b, side)
            await_unit(unit)
            for way in range(2):
                far_copy(way, chain(d, sign), 0, side, unit).start()


    def attend(picks, heads):
        key = jnp.concatenate([units[u, :HALF, :] for u in picks], axis=1)
        val = jnp.concatenate([units[u, HALF:, :] for u in picks], axis=0)
        one = jnp.concatenate([ones[u] for u in picks], axis=0)
        both = jnp.concatenate([val, one], axis=1)
        def score(r):
            return jnp.dot(q_scr[r], key, preferred_element_type=jnp.float32)

        heads = list(heads)
        raw = score(heads[0])
        ready = jnp.exp2(raw).astype(jnp.bfloat16)
        raw = score(heads[1])
        for at, r in enumerate(heads):
            weights = ready
            if at + 1 < len(heads):
                ready = jnp.exp2(raw).astype(jnp.bfloat16)
            if at + 2 < len(heads):
                raw = score(heads[at + 2])
            acc[r] += jnp.dot(weights, both, preferred_element_type=jnp.float32)

    def lookup(i):
        code = jnp.int32(0)
        for at, (d, sign, k, step) in enumerate(ORDER):
            code = jnp.where(i == at, ((d * 2 + sign) * 5 + k) * 4 + step, code)
        step, rest = code % 4, code // 4
        k, rest = rest % 5, rest // 5
        return rest // 2, rest % 2, k, step

    def picks_of(i):
        d, sign, k, step = lookup(i)
        s, low, high = source(d, sign), (b + RING - k) % RING, (b + k) % RING
        last = k // 4
        second = last * b + (1 - last) * high
        return [unit_at(s, at, side) for at in (low, second) for side in range(2)]

    def exchange(i):
        d, sign, k, step = lookup(i)
        s, low, high = source(d, sign), (b + RING - k) % RING, (b + k) % RING
        for side in range(2):
            for way, at in enumerate((low, high)):
                unit = unit_at(s, at, side)

                @pl.when(jnp.logical_or(k < 4, side == way))
                def _():
                    await_unit(unit)

                @pl.when(jnp.logical_or(k < 3, jnp.logical_and(k == 3, side == way)))
                def _():
                    far_copy(way, chain(d, sign), k, side, unit).start()

        @pl.when(step == 1)
        def _():
            arrive(1, 1)
            arrive(1, 0)
            arrive(2, 0)

    def event(i, carry):
        exchange(i)
        attend(picks_of(i), range(8))
        return carry

    def late_event(i, carry):
        exchange(i)
        attend(picks_of(i), range(4, 8))
        return carry

    def early_event(i, carry):
        exchange(i)
        attend(picks_of(i), range(4))
        return carry

    lax.fori_loop(0, EARLY, early_event, 0)
    q_swap.wait_recv()
    attend([u for i in range(EARLY) for u in picks_of(i)], range(4, 8))
    lax.fori_loop(EARLY, 16 - LATE, event, 0)
    lax.fori_loop(16 - LATE, 16, late_event, 0)

    small = lax.broadcasted_iota(jnp.int32, (BLOCK, HEAD_DIM), 1) // 32
    sums = acc[4, :, HEAD_DIM:]
    for r in range(Q_PER_KV):
        o_give[:, r * HEAD_DIM:(r + 1) * HEAD_DIM] = acc[4 + r, :, :HEAD_DIM].astype(jnp.bfloat16)
        sums = jnp.where(small == r, acc[4 + r, :, HEAD_DIM:], sums)
    o_give[:, 4 * HEAD_DIM:] = sums.astype(jnp.bfloat16)
    o_swaps = [
        remote(o_give.at[low:high, :], o_take.at[low:high, :], pair_send.at[at],
               pair_recv.at[at], to_pair)
        for at, (low, high) in enumerate(((128, 192), (192, 256), (0, 128)), 1)
    ]
    for copy in o_swaps:
        copy.start()

    def settle(j, carry):
        d = (j + 1) // 2
        sign = jnp.where(j > 0, (j + 1) % 2, 0)
        s = source(d, sign)
        for side in range(2):
            unit = unit_at(s, b, side)
            for way in range(2):
                for k in range(4 if side == way else 3):
                    far_copy(way, j, k, side, unit).wait_send()
            for way in range(3):
                @pl.when(j == 0)
                def _():
                    near_copy(way, side, unit).wait_send()
        return carry

    def catch_up(i, carry):
        first = 16 - LATE + 2 * i
        attend(picks_of(first) + picks_of(first + 1), range(4))
        return carry

    lax.fori_loop(0, LATE // 2, catch_up, 0)
    lax.fori_loop(0, 4, settle, 0)
    for copy in tok_copies + shares + [q_swap]:
        copy.wait_send()
    loads[7].wait()

    def combine(low, high):
        rows = slice(low, high)
        for r in range(Q_PER_KV):
            span = slice(r * HEAD_DIM, (r + 1) * HEAD_DIM)
            lane_at = 4 * HEAD_DIM + 32 * r
            total = acc[r, rows, HEAD_DIM:] + o_take[
                rows, lane_at:lane_at + 1].astype(jnp.float32)
            att[rows, span] = (
                (acc[r, rows, :HEAD_DIM] + o_take[rows, span].astype(jnp.float32)) / total
            ).astype(jnp.bfloat16)

    def mix(low, high):
        return jnp.dot(att[low * ROWS:high * ROWS, :], w_out[...],
                       preferred_element_type=jnp.float32)

    def part_of(ref, low, high):
        return ref.at[low * ROWS:high * ROWS, :]

    o_swaps[0].wait_recv()
    combine(128, 192)
    both = mix(4, 6)
    give[3 * ROWS:, :] = both[ROWS:].astype(jnp.bfloat16)
    swap_far = remote(part_of(give, 3, 4), part_of(take, 3, 4), end_send.at[0],
                      end_recv.at[0], to_mate)
    swap_far.start()
    swap_far.wait_recv()
    ship[2 * ROWS:, :] = (both[:ROWS] + take[3 * ROWS:, :].astype(jnp.float32)).astype(jnp.bfloat16)
    out_far = remote(part_of(ship, 2, 3), landed.at[0], end_send.at[1], end_recv.at[1],
                     along_x(x_far))
    out_far.start()

    o_swaps[1].wait_recv()
    combine(192, 256)
    give[:2 * ROWS, :] = mix(6, 8).astype(jnp.bfloat16)
    o_swaps[2].wait_recv()
    combine(0, 128)
    front = mix(0, 4)
    give[2 * ROWS:3 * ROWS, :] = front[:ROWS].astype(jnp.bfloat16)
    swap = remote(part_of(give, 0, 3), part_of(take, 0, 3), end_send.at[2], end_recv.at[2],
                  to_mate)
    swap.start()
    swap.wait_recv()
    near = front[ROWS:] + take[:3 * ROWS, :].astype(jnp.float32)
    ship[:2 * ROWS, :] = near[:2 * ROWS].astype(jnp.bfloat16)
    out_up = remote(part_of(ship, 0, 1), landed.at[1], end_send.at[3], end_recv.at[3],
                    along_x(x_up))
    out_down = remote(part_of(ship, 1, 2), landed.at[2], end_send.at[4], end_recv.at[4],
                      along_x(x_down))
    out_up.start()
    out_down.start()
    total = near[2 * ROWS:]
    for copy in o_swaps + [swap_far, swap]:
        copy.wait_send()
    for i, copy in enumerate((out_far, out_up, out_down)):
        copy.wait_recv()
        total = total + landed[i].astype(jnp.float32)
    for copy in (out_far, out_up, out_down):
        copy.wait_send()
    out_ref[...] = total.astype(jnp.bfloat16)


def on_device(tokens, valid_len, norm_gain, w_query, w_key, w_value, q_gain, k_gain, w_out):
    vmem = pl.BlockSpec(memory_space=pltpu.VMEM)
    smem = pl.BlockSpec(memory_space=pltpu.SMEM)
    hbm = pl.BlockSpec(memory_space=pl.ANY)
    dma = pltpu.SemaphoreType.DMA
    bf16, f32 = jnp.bfloat16, jnp.float32
    n_units = RING * RING
    return pl.pallas_call(
        kernel,
        out_shape=pltpu.VMEM(tokens.shape, bf16),
        in_specs=[smem] + [hbm] * 8,
        out_specs=vmem,
        scratch_shapes=[
            pltpu.VMEM(tokens.shape, bf16),
            pltpu.VMEM((1, MODEL), f32),
            pltpu.VMEM((1, HEAD_DIM), f32),
            pltpu.VMEM((1, HEAD_DIM), f32),
            pltpu.VMEM((BLOCK, MODEL), bf16),
            pltpu.VMEM((n_units, BLOCK, HEAD_DIM), bf16),
            pltpu.VMEM((n_units, HALF, HEAD_DIM), bf16),
            pltpu.VMEM((2 * Q_PER_KV, BLOCK, HEAD_DIM), bf16),
            pltpu.VMEM((2 * Q_PER_KV, BLOCK, 2 * HEAD_DIM), f32),
            pltpu.VMEM((BLOCK, Q_PER_KV * HEAD_DIM), bf16),
            pltpu.VMEM((3, BLOCK, HEAD_DIM), f32),
            pltpu.VMEM(w_query.shape, bf16),
            pltpu.VMEM(w_key.shape, bf16),
            pltpu.VMEM(w_value.shape, bf16),
            pltpu.VMEM(w_out.shape, bf16),
            pltpu.VMEM((BLOCK, 5 * HEAD_DIM), bf16),
            pltpu.VMEM((BLOCK, 5 * HEAD_DIM), bf16),
            pltpu.VMEM((HALF, MODEL), bf16),
            pltpu.VMEM((HALF, MODEL), bf16),
            pltpu.VMEM((3 * ROWS, MODEL), bf16),
            pltpu.VMEM((3, ROWS, MODEL), bf16),
            dma((8,)), dma((8,)), dma((8,)), dma((n_units,)), dma((8,)), dma((72,)),
            dma((4,)), dma((4,)), dma((5,)), dma((5,)),
        ],
        compiler_params=pltpu.CompilerParams(
            collective_id=0, has_side_effects=True, vmem_limit_bytes=60 * 1024 * 1024),
    )(valid_len, tokens, norm_gain[None, :], q_gain[None, :], k_gain[None, :], w_query, w_key,
      w_value, w_out)


def solution(mesh):
    return jax.shard_map(
        on_device,
        mesh=mesh,
        in_specs=(
            P(("sp", "tp"), None),
            P(),
            P(),
            P(None, "tp"),
            P(None, "tp"),
            P(None, "tp"),
            P(),
            P(),
            P("tp", None),
        ),
        out_specs=P(("sp", "tp"), None),
        check_vma=False,
    )
```

```python
import functools
import math

import jax
import jax.numpy as jnp
from jax import lax
from jax.experimental import pallas as pl
from jax.experimental.pallas import tpu as pltpu
from jax.sharding import PartitionSpec as P

HEAD_DIM = 128
Q_PER_KV = 4
GRID_W = 64
ROWS = 32
BLOCK = 256
HALF = 128
RING = 8
MODEL = 1024

LATE = 6
EARLY = 1
ORDER = [
    (0, 0, 1, 1), (1, 1, 1, 0), (1, 0, 1, 0), (2, 0, 1, 0),
    (0, 0, 2, 0), (1, 1, 2, 0), (1, 0, 2, 0), (2, 0, 2, 0),
    (0, 0, 3, 0), (1, 1, 3, 0), (1, 0, 3, 0), (2, 0, 3, 0),
    (0, 0, 4, 0), (1, 1, 4, 0), (1, 0, 4, 0), (2, 0, 4, 0),
]

norm_eps = 1e-06
rope_base = 10000.0
MESH = pl.DeviceIdType.MESH


def unit_rows(rows, gain):
    wide = rows.astype(jnp.float32)
    scale = lax.rsqrt(jnp.mean(wide * wide, axis=-1, keepdims=True) + norm_eps)
    return (wide * scale * gain).astype(jnp.bfloat16)


def rotate(part, tables):
    width = part.shape[-1]
    scale = lax.rsqrt(jnp.mean(part * part, axis=-1, keepdims=True) + norm_eps)
    ahead = pltpu.roll(part, width // 4, 1)
    behind = pltpu.roll(part, width - width // 4, 1)
    return (part * tables[0] + ahead * tables[1] + behind * tables[2]) * scale


def kernel(valid_ref, own_hbm, gain_hbm, q_gain_hbm, k_gain_hbm, w_query_hbm, w_key_hbm,
           w_value_hbm, w_out_hbm, out_ref,
           own, gain, q_gain, k_gain, tok, units, ones, q_scr, acc, att, tabs,
           w_query, w_key, w_value, w_out, o_give, o_take, give, take, ship, landed,
           load_sem, tok_send, tok_recv, unit_recv, near_send, far_send, pair_send, pair_recv,
           end_send, end_recv):
    me = lax.axis_index("sp")
    tp = lax.axis_index("tp")
    z, y = me // RING, me % RING
    x, core = tp // 2, tp % 2
    x_up, x_down, x_far = (x + 1) % 4, (x + 3) % 4, (x + 2) % 4
    to_mate = {"sp": me, "tp": 2 * x + 1 - core}
    a = core * y + (1 - core) * z
    b = core * z + (1 - core) * y
    parity, group = a % 2, a // 2

    def block_at(a_at, b_at):
        return (1 - core) * (a_at * RING + b_at) + core * (b_at * RING + a_at)

    def along_x(at):
        return {"sp": me, "tp": 2 * at + core}

    def along(a_at, b_at):
        return {"sp": block_at(a_at, b_at), "tp": tp}

    to_near = [along(2 * ((group + ahead) % 4) + parity, b) for ahead in (1, 3, 2)]
    to_far = [along(a, (b + 1) % RING), along(a, (b + RING - 1) % RING)]
    to_pair = along(a + 1 - 2 * parity, b)

    barrier = pltpu.get_barrier_semaphore()
    friends = [to_mate, along_x(x_far), along_x(x_up), along_x(x_down), to_pair]
    friends += to_near + to_far
    for friend in friends:
        pl.semaphore_signal(barrier, inc=1, device_id=friend, device_id_type=MESH)

    loads = [
        pltpu.make_async_copy(src, dst, load_sem.at[i])
        for i, (src, dst) in enumerate([
            (own_hbm, own), (gain_hbm, gain), (k_gain_hbm, k_gain), (q_gain_hbm, q_gain),
            (w_key_hbm, w_key), (w_value_hbm, w_value), (w_query_hbm, w_query),
            (w_out_hbm, w_out)])
    ]
    for load in loads:
        load.start()
    loads[0].wait()
    pl.semaphore_wait(barrier, len(friends))

    def remote(source, target, send, recv, device):
        return pltpu.make_async_remote_copy(
            src_ref=source, dst_ref=target, send_sem=send, recv_sem=recv,
            device_id=device, device_id_type=MESH)

    def slot(at):
        return tok.at[at * ROWS:(at + 1) * ROWS, :]

    tok_up = remote(own, slot(2), tok_send.at[0], tok_recv.at[0], along_x(x_up))
    tok_down = remote(own, slot(1), tok_send.at[1], tok_recv.at[1], along_x(x_down))
    tok_mate = remote(own, slot(0), tok_send.at[2], tok_recv.at[2], to_mate)
    tok_far = remote(own, slot(4), tok_send.at[3], tok_recv.at[3], along_x(x_far))
    tok_copies = [tok_up, tok_down, tok_mate, tok_far]
    for copy in tok_copies:
        copy.start()
    tok[3 * ROWS:4 * ROWS, :] = own[...]

    def place(line):
        at = line // ROWS
        ahead = jnp.where(jnp.logical_or(at == 1, at == 6), 1, 0)
        ahead = jnp.where(jnp.logical_or(at == 2, at == 7), 3, ahead)
        ahead = jnp.where(jnp.logical_or(at == 4, at == 5), 2, ahead)
        side = jnp.where(jnp.logical_and(at > 0, at < 5), core, 1 - core)
        return (x + ahead) % 4, side * ROWS + line % ROWS

    lane = lax.broadcasted_iota(jnp.int32, (BLOCK, HEAD_DIM), 1)
    line = lax.broadcasted_iota(jnp.int32, (BLOCK, HEAD_DIM), 0)
    grid_row, grid_col = place(line)
    spot = jnp.where(lane < HEAD_DIM // 2, me * 4 + grid_row, grid_col).astype(jnp.float32)
    exponent = (lane % 32).astype(jnp.float32) * (-2.0 / 64 * math.log2(rope_base))
    angle = spot * jnp.exp2(exponent)
    cosine, sine = jnp.cos(angle), jnp.sin(angle)
    second = (lane // 32) % 2 == 1
    tabs[0] = cosine
    tabs[1] = jnp.where(second, sine, 0.0)
    tabs[2] = jnp.where(second, 0.0, -sine)

    valid = valid_ref[0]
    spread = []
    for side in range(2):
        short = lax.broadcasted_iota(jnp.int32, (HALF, HEAD_DIM), 0) + side * HALF
        high, low = place(short)
        spread.append(high * GRID_W + low)
    def fill(i, carry):
        p = block_at(2 * (i // RING) + parity, i % RING)
        for side in range(2):
            kept = spread[side] + p * BLOCK < valid
            ones[2 * i + side] = jnp.where(kept, 1.0, 0.0).astype(jnp.bfloat16)
        return carry

    lax.fori_loop(0, 4 * RING, fill, 0)
    acc[...] = jnp.zeros_like(acc)

    def share(ours, theirs, at):
        return remote(slot(ours), slot(theirs), tok_send.at[at], tok_recv.at[at], to_mate)

    shares = [share(2, 7, 4), share(1, 6, 5), share(4, 5, 6)]
    for copy, onward in zip((tok_up, tok_down), shares):
        copy.wait_recv()
        onward.start()
    tok_mate.wait_recv()

    for i in range(1, 6):
        loads[i].wait()

    def turns(table, side):
        wide = jnp.broadcast_to(table, (8, HEAD_DIM))
        moved = [wide, pltpu.roll(wide, 32, 1), pltpu.roll(wide, HEAD_DIM - 32, 1)]
        rows = slice(side * HALF, (side + 1) * HALF)
        return [tabs[i, rows, :] * moved[i][:1, :] for i in range(3)]

    def unit_at(group_at, b_at, side):
        return (group_at * RING + b_at) * 2 + side

    def relay(unit, device, send):
        return remote(units.at[unit], units.at[unit], send, unit_recv.at[unit], device)

    def await_unit(unit):
        relay(unit, to_mate, near_send.at[0]).wait_recv()

    def near_copy(way, side, unit):
        return relay(unit, to_near[way], near_send.at[way * 2 + side])

    def far_copy(way, j, k, side, unit):
        return relay(unit, to_far[way], far_send.at[((way * 4 + j) * 4 + k) * 2 + side])

    def project(side):
        rows = slice(side * HALF, (side + 1) * HALF)
        normed = unit_rows(tok[rows, :], gain[...])
        keys = rotate(jnp.dot(normed, w_key[...], preferred_element_type=jnp.float32),
                      turns(k_gain[...], side))
        values = jnp.dot(normed, w_value[...], preferred_element_type=jnp.float32)
        kept = spread[side] + me * BLOCK < valid
        unit = unit_at(group, b, side)
        units[unit, :HALF, :] = keys.T.astype(jnp.bfloat16)
        units[unit, HALF:, :] = jnp.where(kept, values, 0.0).astype(jnp.bfloat16)
        for way in range(2):
            far_copy(way, 0, 0, side, unit).start()
        for way in (0, 1, 2):
            near_copy(way, side, unit).start()
        return normed

    def queries(normed, side):
        rows = slice(side * HALF, (side + 1) * HALF)
        factor = HEAD_DIM ** (-0.5) * math.log2(math.e)
        tables = turns(q_gain[...] * factor, side)
        projected = jnp.dot(normed, w_query[...], preferred_element_type=jnp.float32)
        for r in range(Q_PER_KV):
            head = rotate(projected[:, r * HEAD_DIM:(r + 1) * HEAD_DIM], tables)
            q_scr[r, rows, :] = head.astype(jnp.bfloat16)

    first = project(0)
    tok_far.wait_recv()
    shares[2].start()
    loads[6].wait()
    queries(first, 0)
    for copy in shares:
        copy.wait_recv()
    other = project(1)
    queries(other, 1)
    q_swap = remote(q_scr.at[pl.ds(0, 4)], q_scr.at[pl.ds(4, 4)], pair_send.at[0],
                    pair_recv.at[0], to_pair)
    q_swap.start()

    def chain(d, sign):
        return jnp.maximum(2 * d - 1 + sign, 0)

    def source(d, sign):
        return (group + d * (2 * sign - 1) + 4) % 4

    def arrive(d, sign):
        for side in range(2):
            unit = unit_at(source(d, sign), b, side)
            await_unit(unit)
            for way in range(2):
                far_copy(way, chain(d, sign), 0, side, unit).start()


    def attend(picks, heads):
        key = jnp.concatenate([units[u, :HALF, :] for u in picks], axis=1)
        val = jnp.concatenate([units[u, HALF:, :] for u in picks], axis=0)
        one = jnp.concatenate([ones[u] for u in picks], axis=0)
        both = jnp.concatenate([val, one], axis=1)
        def score(r):
            return jnp.dot(q_scr[r], key, preferred_element_type=jnp.float32)

        heads = list(heads)
        raw = score(heads[0])
        ready = jnp.exp2(raw).astype(jnp.bfloat16)
        raw = score(heads[1])
        for at, r in enumerate(heads):
            weights = ready
            if at + 1 < len(heads):
                ready = jnp.exp2(raw).astype(jnp.bfloat16)
            if at + 2 < len(heads):
                raw = score(heads[at + 2])
            acc[r] += jnp.dot(weights, both, preferred_element_type=jnp.float32)

    def lookup(i):
        code = jnp.int32(0)
        for at, (d, sign, k, step) in enumerate(ORDER):
            code = jnp.where(i == at, ((d * 2 + sign) * 5 + k) * 4 + step, code)
        step, rest = code % 4, code // 4
        k, rest = rest % 5, rest // 5
        return rest // 2, rest % 2, k, step

    def picks_of(i):
        d, sign, k, step = lookup(i)
        s, low, high = source(d, sign), (b + RING - k) % RING, (b + k) % RING
        last = k // 4
        second = last * b + (1 - last) * high
        return [unit_at(s, at, side) for at in (low, second) for side in range(2)]

    def exchange(i):
        d, sign, k, step = lookup(i)
        s, low, high = source(d, sign), (b + RING - k) % RING, (b + k) % RING
        for side in range(2):
            for way, at in enumerate((low, high)):
                unit = unit_at(s, at, side)

                @pl.when(jnp.logical_or(k < 4, side == way))
                def _():
                    await_unit(unit)

                @pl.when(jnp.logical_or(k < 3, jnp.logical_and(k == 3, side == way)))
                def _():
                    far_copy(way, chain(d, sign), k, side, unit).start()

        @pl.when(step == 1)
        def _():
            arrive(1, 1)
            arrive(1, 0)
            arrive(2, 0)

    def event(i, carry):
        exchange(i)
        attend(picks_of(i), range(8))
        return carry

    def late_event(i, carry):
        exchange(i)
        attend(picks_of(i), range(4, 8))
        return carry

    def early_event(i, carry):
        exchange(i)
        attend(picks_of(i), range(4))
        return carry

    lax.fori_loop(0, EARLY, early_event, 0)
    q_swap.wait_recv()
    attend([u for i in range(EARLY) for u in picks_of(i)], range(4, 8))
    lax.fori_loop(EARLY, 16 - LATE, event, 0)
    lax.fori_loop(16 - LATE, 16, late_event, 0)

    small = lax.broadcasted_iota(jnp.int32, (BLOCK, HEAD_DIM), 1) // 32
    sums = acc[4, :, HEAD_DIM:]
    for r in range(Q_PER_KV):
        o_give[:, r * HEAD_DIM:(r + 1) * HEAD_DIM] = acc[4 + r, :, :HEAD_DIM].astype(jnp.bfloat16)
        sums = jnp.where(small == r, acc[4 + r, :, HEAD_DIM:], sums)
    o_give[:, 4 * HEAD_DIM:] = sums.astype(jnp.bfloat16)
    o_swaps = [
        remote(o_give.at[low:high, :], o_take.at[low:high, :], pair_send.at[at],
               pair_recv.at[at], to_pair)
        for at, (low, high) in enumerate(((128, 192), (192, 256), (0, 128)), 1)
    ]
    for copy in o_swaps:
        copy.start()

    def settle(j, carry):
        d = (j + 1) // 2
        sign = jnp.where(j > 0, (j + 1) % 2, 0)
        s = source(d, sign)
        for side in range(2):
            unit = unit_at(s, b, side)
            for way in range(2):
                for k in range(4 if side == way else 3):
                    far_copy(way, j, k, side, unit).wait_send()
            for way in range(3):
                @pl.when(j == 0)
                def _():
                    near_copy(way, side, unit).wait_send()
        return carry

    def catch_up(i, carry):
        first = 16 - LATE + 2 * i
        attend(picks_of(first) + picks_of(first + 1), range(4))
        return carry

    lax.fori_loop(0, LATE // 2, catch_up, 0)
    lax.fori_loop(0, 4, settle, 0)
    for copy in tok_copies + shares + [q_swap]:
        copy.wait_send()
    loads[7].wait()

    def combine(low, high):
        rows = slice(low, high)
        for r in range(Q_PER_KV):
            span = slice(r * HEAD_DIM, (r + 1) * HEAD_DIM)
            lane_at = 4 * HEAD_DIM + 32 * r
            total = acc[r, rows, HEAD_DIM:] + o_take[
                rows, lane_at:lane_at + 1].astype(jnp.float32)
            att[rows, span] = (
                (acc[r, rows, :HEAD_DIM] + o_take[rows, span].astype(jnp.float32)) / total
            ).astype(jnp.bfloat16)

    def mix(low, high):
        return jnp.dot(att[low * ROWS:high * ROWS, :], w_out[...],
                       preferred_element_type=jnp.float32)

    def part_of(ref, low, high):
        return ref.at[low * ROWS:high * ROWS, :]

    o_swaps[0].wait_recv()
    combine(128, 192)
    both = mix(4, 6)
    give[3 * ROWS:, :] = both[ROWS:].astype(jnp.bfloat16)
    swap_far = remote(part_of(give, 3, 4), part_of(take, 3, 4), end_send.at[0],
                      end_recv.at[0], to_mate)
    swap_far.start()
    swap_far.wait_recv()
    ship[2 * ROWS:, :] = (both[:ROWS] + take[3 * ROWS:, :].astype(jnp.float32)).astype(jnp.bfloat16)
    out_far = remote(part_of(ship, 2, 3), landed.at[0], end_send.at[1], end_recv.at[1],
                     along_x(x_far))
    out_far.start()

    o_swaps[1].wait_recv()
    combine(192, 256)
    give[:2 * ROWS, :] = mix(6, 8).astype(jnp.bfloat16)
    o_swaps[2].wait_recv()
    combine(0, 128)
    front = mix(0, 4)
    give[2 * ROWS:3 * ROWS, :] = front[:ROWS].astype(jnp.bfloat16)
    swap = remote(part_of(give, 0, 3), part_of(take, 0, 3), end_send.at[2], end_recv.at[2],
                  to_mate)
    swap.start()
    swap.wait_recv()
    near = front[ROWS:] + take[:3 * ROWS, :].astype(jnp.float32)
    ship[:2 * ROWS, :] = near[:2 * ROWS].astype(jnp.bfloat16)
    out_up = remote(part_of(ship, 0, 1), landed.at[1], end_send.at[3], end_recv.at[3],
                    along_x(x_up))
    out_down = remote(part_of(ship, 1, 2), landed.at[2], end_send.at[4], end_recv.at[4],
                      along_x(x_down))
    out_up.start()
    out_down.start()
    total = near[2 * ROWS:]
    for copy in o_swaps + [swap_far, swap]:
        copy.wait_send()
    for i, copy in enumerate((out_far, out_up, out_down)):
        copy.wait_recv()
        total = total + landed[i].astype(jnp.float32)
    for copy in (out_far, out_up, out_down):
        copy.wait_send()
    out_ref[...] = total.astype(jnp.bfloat16)


def on_device(tokens, valid_len, norm_gain, w_query, w_key, w_value, q_gain, k_gain, w_out):
    vmem = pl.BlockSpec(memory_space=pltpu.VMEM)
    smem = pl.BlockSpec(memory_space=pltpu.SMEM)
    hbm = pl.BlockSpec(memory_space=pl.ANY)
    dma = pltpu.SemaphoreType.DMA
    bf16, f32 = jnp.bfloat16, jnp.float32
    n_units = RING * RING
    return pl.pallas_call(
        kernel,
        out_shape=pltpu.VMEM(tokens.shape, bf16),
        in_specs=[smem] + [hbm] * 8,
        out_specs=vmem,
        scratch_shapes=[
            pltpu.VMEM(tokens.shape, bf16),
            pltpu.VMEM((1, MODEL), f32),
            pltpu.VMEM((1, HEAD_DIM), f32),
            pltpu.VMEM((1, HEAD_DIM), f32),
            pltpu.VMEM((BLOCK, MODEL), bf16),
            pltpu.VMEM((n_units, BLOCK, HEAD_DIM), bf16),
            pltpu.VMEM((n_units, HALF, HEAD_DIM), bf16),
            pltpu.VMEM((2 * Q_PER_KV, BLOCK, HEAD_DIM), bf16),
            pltpu.VMEM((2 * Q_PER_KV, BLOCK, 2 * HEAD_DIM), f32),
            pltpu.VMEM((BLOCK, Q_PER_KV * HEAD_DIM), bf16),
            pltpu.VMEM((3, BLOCK, HEAD_DIM), f32),
            pltpu.VMEM(w_query.shape, bf16),
            pltpu.VMEM(w_key.shape, bf16),
            pltpu.VMEM(w_value.shape, bf16),
            pltpu.VMEM(w_out.shape, bf16),
            pltpu.VMEM((BLOCK, 5 * HEAD_DIM), bf16),
            pltpu.VMEM((BLOCK, 5 * HEAD_DIM), bf16),
            pltpu.VMEM((HALF, MODEL), bf16),
            pltpu.VMEM((HALF, MODEL), bf16),
            pltpu.VMEM((3 * ROWS, MODEL), bf16),
            pltpu.VMEM((3, ROWS, MODEL), bf16),
            dma((8,)), dma((8,)), dma((8,)), dma((n_units,)), dma((8,)), dma((72,)),
            dma((4,)), dma((4,)), dma((5,)), dma((5,)),
        ],
        compiler_params=pltpu.CompilerParams(
            collective_id=0, has_side_effects=True, vmem_limit_bytes=60 * 1024 * 1024),
    )(valid_len, tokens, norm_gain[None, :], q_gain[None, :], k_gain[None, :], w_query, w_key,
      w_value, w_out)


def solution(mesh):
    return jax.shard_map(
        on_device,
        mesh=mesh,
        in_specs=(
            P(("sp", "tp"), None),
            P(),
            P(),
            P(None, "tp"),
            P(None, "tp"),
            P(None, "tp"),
            P(),
            P(),
            P("tp", None),
        ),
        out_specs=P(("sp", "tp"), None),
        check_vma=False,
    )
```
